512 devices in a mesh: sp: 16 (over z), dp: 32 (over y, x, core).
Axes of the slice: x: 4, y: 4, z: 16, core: 2. Of those that a mesh axis runs over, the one named last changes fastest.
Arguments:
- stream_x: bfloat16 [32, 2048, 2048], P('dp', 'sp'), may hold values from -6 to 6
- stream_b: bfloat16 [32, 2048, 1024], P('dp', 'sp'), may hold values from -6 to 6
- stream_c: bfloat16 [32, 2048, 1024], P('dp', 'sp'), may hold values from -6 to 6
- gate_z: bfloat16 [32, 2048, 2048], P('dp', 'sp'), may hold values from -6 to 6
- step_raw: bfloat16 [32, 2048, 32], P('dp', 'sp'), may hold values from -4 to 3
- conv_x: bfloat16 [4, 2048], P(None, 'sp'), may hold values from -3 to 3
- conv_b: bfloat16 [4, 1024], replicated, may hold values from -3 to 3
- conv_c: bfloat16 [4, 1024], replicated, may hold values from -3 to 3
- decay_log: float32 [32], P('sp'), may hold values from -20 to 0
- norm_gain: float32 [2048], replicated, may hold values from 0.1 to 1.9
- w_out: bfloat16 [2048, 2048], P('dp'), may hold values from -0.125 to 0.125
Outputs:
- mixed: bfloat16 [32, 2048, 2048], P('dp', 'sp')
The draws below stay inside these ranges and needn't reach their ends.
All inputs are finite; a program needn't handle non-finite values.
Results may differ from the reference program's by a relative error of at most 0.011.
Values may be sent and summed in bfloat16 or wider, within the bound.
No kernel may reach another device: no remote copies, remote signals or barrier semaphores. Data moves between devices by JAX's collectives and lax.ppermute only.
A program may use at most 64 MiB of HBM per device.

```python
import jax
import jax.numpy as jnp
from jax import lax

D = 2048
HEADS = 32
HEAD_DIM = 64
STATE = 128
CONV = 4
BLOCK = 64
TOK_DEV = 128
DI = 2048
GROUP_STATE = 1024
SEQS = 32
LEN = 2048


def draw_step_raw(key, part):
    first_key, second_key = jax.random.split(jax.random.fold_in(key, 11))
    noise = jnp.clip(jax.random.normal(first_key, (SEQS, LEN, HEADS), jnp.float32), -3.0, 3.0)
    offset = jax.random.uniform(second_key, (SEQS, LEN // TOK_DEV, 1, HEADS), jnp.float32, -2.0, 1.0)
    offset = jnp.broadcast_to(offset, (SEQS, LEN // TOK_DEV, TOK_DEV, HEADS)).reshape(SEQS, LEN, HEADS)
    return (0.6 * noise + offset).astype(jnp.bfloat16)


def draw_decay_log(key, part):
    pick_key, slow_key, quick_key = jax.random.split(jax.random.fold_in(key, 23), 3)
    chance = 0.5
    quick_heads = jax.random.uniform(pick_key, (HEADS,), jnp.float32) < chance
    slow_rate = jax.random.uniform(slow_key, (HEADS,), jnp.float32, 0.3, 1.0) / LEN
    quick_rate = jax.random.uniform(quick_key, (HEADS,), jnp.float32, 0.03, 0.08)
    return jnp.log(jnp.where(quick_heads, quick_rate, slow_rate)).astype(jnp.float32)


def shard_levels(key, dims, cuts, least, largest):
    factor_of, own = 1.0, jax.random.fold_in(key, 6)
    for position, blocks in cuts:
        heights = jnp.exp(jax.random.uniform(jax.random.fold_in(own, position), (blocks,), jnp.float32, least / len(cuts), largest / len(cuts)))
        factor_of = factor_of * jnp.repeat(heights, dims[position] // blocks).reshape([-1 if axis == position else 1 for axis in range(len(dims))])
    return factor_of


def scatter_about(own_key, extent, scale, limit, shards=(), dtype=jnp.bfloat16):
    factor_of = shard_levels(own_key, extent, shards, -0.22, 0.18) if shards else 1.0
    drawn = jax.random.normal(own_key, extent, jnp.float32) * scale * factor_of
    return jnp.minimum(jnp.maximum(drawn, -limit), limit).astype(dtype)


def setup_inputs(seed: int = 0) -> dict:
    seeds = jax.random.split(jax.random.key(seed), 12)
    return {
        "stream_x": scatter_about(seeds[0], (SEQS, LEN, DI), 1.0, 6.0, ((0, 32), (1, 16))),
        "stream_b": scatter_about(seeds[1], (SEQS, LEN, GROUP_STATE), 1.0, 6.0, ((0, 32), (1, 16))),
        "stream_c": scatter_about(seeds[2], (SEQS, LEN, GROUP_STATE), 1.0, 6.0, ((0, 32), (1, 16))),
        "gate_z": scatter_about(seeds[3], (SEQS, LEN, DI), 1.0, 6.0, ((0, 32), (1, 16))),
        "step_raw": draw_step_raw(jax.random.fold_in(seeds[11], 71), 0),
        "conv_x": scatter_about(seeds[5], (CONV, DI), CONV ** -0.5, 3.0, ((1, 16),)),
        "conv_b": scatter_about(seeds[6], (CONV, GROUP_STATE), CONV ** -0.5, 3.0),
        "conv_c": scatter_about(seeds[7], (CONV, GROUP_STATE), CONV ** -0.5, 3.0),
        "decay_log": draw_decay_log(jax.random.fold_in(seeds[11], 71), 0),
        "norm_gain": jnp.clip(1.0 + 0.18 * jax.random.normal(seeds[9], (DI,), jnp.float32), 0.1, 1.9),
        "w_out": scatter_about(seeds[10], (DI, D), DI ** -0.5, 0.125, ((0, 32),)),
    }


NORM_EPS = 1.0

def causal_conv(sequence, kernel):
    taps = kernel.shape[0]
    length = sequence.shape[0]
    padded = jnp.pad(sequence.astype(jnp.float32), ((taps - 1, 0), (0, 0)))
    summed = jnp.zeros(sequence.shape, jnp.float32)
    for tap_index in range(taps):
        summed = summed + kernel[tap_index].astype(jnp.float32) * padded[tap_index:tap_index + length]
    rounded = lax.optimization_barrier(jax.nn.silu(summed).astype(jnp.bfloat16))
    return rounded.astype(jnp.float32)

def mixer(seq_x, seq_b, seq_c, seq_raw, conv_x, conv_b, conv_c, decay_log):
    length = seq_x.shape[0]
    head_count = seq_raw.shape[1]
    group_count = seq_b.shape[1] // STATE
    ratio = head_count // group_count
    blocks = length // BLOCK
    highest = lax.Precision.HIGHEST
    x_values = causal_conv(seq_x, conv_x).reshape(blocks, BLOCK, group_count, ratio, HEAD_DIM)
    b_values = causal_conv(seq_b, conv_b).reshape(blocks, BLOCK, group_count, STATE)
    c_values = causal_conv(seq_c, conv_c).reshape(blocks, BLOCK, group_count, STATE)
    step_size = jax.nn.softplus(seq_raw.astype(jnp.float32))
    log_decay = (step_size * (-jnp.exp(decay_log))[None, :]).reshape(blocks, BLOCK, group_count, ratio)
    step_size = step_size.reshape(blocks, BLOCK, group_count, ratio)
    cumul = jnp.cumsum(log_decay, axis=1)
    scores = jnp.einsum('kTgn,kSgn->kTSg', c_values, b_values, precision=highest)
    causal = jnp.tril(jnp.ones((BLOCK, BLOCK), bool))
    spread = cumul[:, :, None] - cumul[:, None, :]
    decay = jnp.exp(jnp.where(causal[None, :, :, None, None], spread, -jnp.inf))
    weights = scores[..., None] * decay * step_size[:, None]
    inner = jnp.einsum('kTSgr,kSgrp->kTgrp', weights, x_values, precision=highest)
    last = cumul[:, -1]
    tail = jnp.exp(last[:, None] - cumul) * step_size
    local = jnp.einsum('kSgn,kSgr,kSgrp->kgrpn', b_values, tail, x_values, precision=highest)
    before = jnp.cumsum(last, axis=0) - last
    after = before + last
    gap = before[:, None] - after[None, :]
    lower = jnp.tril(jnp.ones((blocks, blocks), bool), -1)
    carry_weight = jnp.exp(jnp.where(lower[:, :, None, None], gap, -jnp.inf))
    entering = jnp.einsum('kjgr,jgrpn->kgrpn', carry_weight, local, precision=highest)
    carried = jnp.einsum('kTgn,kgrpn,kTgr->kTgrp', c_values, entering, jnp.exp(cumul), precision=highest)
    return (inner + carried).reshape(length, head_count * HEAD_DIM).astype(jnp.bfloat16)

def gate_norm(core_out, seq_z, gain, group_width):
    length = core_out.shape[0]
    gated = core_out.astype(jnp.float32) * jax.nn.silu(seq_z.astype(jnp.float32))
    grouped = gated.reshape(length, -1, group_width)
    scale = lax.rsqrt(lax.optimization_barrier(jnp.mean(grouped * grouped, axis=-1, keepdims=True)) + NORM_EPS)
    return ((grouped * scale).reshape(length, -1) * gain[None, :]).astype(jnp.bfloat16)

def reference(stream_x, stream_b, stream_c, gate_z, step_raw, conv_x, conv_b, conv_c, decay_log, norm_gain, w_out):
    group_width = HEAD_DIM

    def one_sequence(inputs):
        seq_x, seq_b, seq_c, seq_z, seq_raw = inputs
        core_out = mixer(seq_x, seq_b, seq_c, seq_raw, conv_x, conv_b, conv_c, decay_log)
        normed = gate_norm(core_out, seq_z, norm_gain, group_width)
        return jnp.dot(normed, w_out, preferred_element_type=jnp.float32).astype(jnp.bfloat16)
    return lax.map(one_sequence, (stream_x, stream_b, stream_c, gate_z, step_raw))
```

```python
import jax
import jax.numpy as jnp
from jax import lax
from jax.experimental import pallas as pl
from jax.experimental.pallas import tpu as pltpu
from jax.sharding import PartitionSpec as P

HEAD_DIM = 64
STATE = 128
RATIO = 4
NORM_EPS = 1.0
HIGHEST = lax.Precision.HIGHEST
F32 = jnp.float32
BF16 = jnp.bfloat16
HALO = 8


def silu(u):
    return 0.5 * u * (1.0 + jnp.tanh(0.5 * u))


def conv_silu(pad_ref, halo, value, taps):
    rows = value.shape[0]
    pad_ref[0:HALO, :] = halo.astype(F32)
    pad_ref[HALO : HALO + rows, :] = value.astype(F32)
    total = taps[3:4, :] * pad_ref[HALO : HALO + rows, :]
    for back in range(1, 4):
        total = total + taps[3 - back : 4 - back, :] * pad_ref[HALO - back : HALO - back + rows, :]
    return silu(total).astype(BF16)


def per_head(columns, first, width):
    tokens = columns.shape[0]
    lane = lax.broadcasted_iota(jnp.int32, (tokens, 128), 1)
    pieces = []
    for pair in range(width // 128):
        left = jnp.broadcast_to(columns[:, first + 2 * pair : first + 2 * pair + 1], (tokens, 128))
        right = jnp.broadcast_to(
            columns[:, first + 2 * pair + 1 : first + 2 * pair + 2], (tokens, 128)
        )
        pieces.append(jnp.where(lane < HEAD_DIM, left, right))
    return jnp.concatenate(pieces, axis=1)


def state_kernel(
    x_ref, b_ref, hx_ref, hb_ref, shared_ref, tb_ref, dt_ref,
    state_ref, xin_ref, bin_ref, cum_ref, padx_ref, padb_ref,
):
    tokens = x_ref.shape[0]
    taps_x = jnp.concatenate([shared_ref[0], shared_ref[1]], axis=1)
    xin = conv_silu(padx_ref, hx_ref[...], x_ref[...], taps_x)
    bin_ = conv_silu(padb_ref, hb_ref[...], b_ref[...], tb_ref[...].astype(F32))
    xin_ref[...] = xin
    bin_ref[...] = bin_
    dt = dt_ref[0]
    logs = jnp.concatenate([shared_ref[0, 4:6, :], shared_ref[1, 4:6, :]], axis=0)
    la = -jnp.exp(logs) * dt
    src = lax.broadcasted_iota(jnp.int32, (tokens, tokens), 0)
    dst = lax.broadcasted_iota(jnp.int32, (tokens, tokens), 1)
    upper = (src <= dst).astype(F32)
    both = jnp.concatenate([la, dt], axis=0)
    summed = jnp.dot(both, upper, precision=HIGHEST, preferred_element_type=F32)
    cum = summed[0:RATIO]
    packed = jnp.concatenate([cum, dt], axis=0)
    cum_ref[0] = packed
    last = cum[:, tokens - 1 : tokens]
    tail = jnp.exp(last - cum) * dt
    tails = jnp.concatenate([tail, tail], axis=0)
    columns = jnp.transpose(tails)
    scaled = (xin.astype(F32) * per_head(columns, 0, RATIO * HEAD_DIM)).astype(BF16)
    state = lax.dot_general(
        scaled, bin_, (((0,), (0,)), ((), ())), preferred_element_type=F32
    )
    state_ref[...] = state.astype(BF16)


def inner_kernel(c_ref, hc_ref, tc_ref, bin_ref, xin_ref, cum_ref, cin_ref, inner_ref, padc_ref):
    tokens = c_ref.shape[0]
    cin = conv_silu(padc_ref, hc_ref[...], c_ref[...], tc_ref[...].astype(F32))
    cin_ref[...] = cin
    scores = lax.dot_general(
        cin, bin_ref[...], (((1,), (1,)), ((), ())), preferred_element_type=F32
    )
    rows = cum_ref[0]
    columns = jnp.transpose(rows)
    row_id = lax.broadcasted_iota(jnp.int32, (tokens, tokens), 0)
    col_id = lax.broadcasted_iota(jnp.int32, (tokens, tokens), 1)
    causal = row_id >= col_id
    for head in range(RATIO):
        spread = columns[:, head : head + 1] - rows[head : head + 1, :]
        decay = jnp.exp(jnp.where(causal, spread, -jnp.inf))
        weights = (scores * decay * rows[RATIO + head : RATIO + head + 1, :]).astype(BF16)
        cols = slice(head * HEAD_DIM, (head + 1) * HEAD_DIM)
        inner_ref[:, cols] = jnp.dot(weights, xin_ref[:, cols], preferred_element_type=F32)


def scan_kernel(decay_ref, local_ref, out_ref):
    count = local_ref.shape[0]
    for head in range(2):
        rows = slice(head * HEAD_DIM, (head + 1) * HEAD_DIM)
        entering = jnp.zeros((HEAD_DIM, STATE), F32)
        for step in range(count):
            out_ref[step, rows, :] = entering.astype(BF16)
            if step + 1 < count:
                entering = entering * decay_ref[step, head] + local_ref[step, rows, :].astype(F32)


def out_kernel(
    ent_ref, cin_ref, inner_ref, cum_ref, z_ref, gain_ref, w_ref, out_ref, acc_ref
):
    group = pl.program_id(0)
    carried = lax.dot_general(
        cin_ref[...], ent_ref[...], (((1,), (1,)), ((), ())), preferred_element_type=F32
    )
    width = RATIO * HEAD_DIM
    columns = jnp.transpose(jnp.exp(cum_ref[0]))
    core = (inner_ref[...] + carried * per_head(columns, 0, width)).astype(BF16)
    v = core.astype(F32) * silu(z_ref[...].astype(F32))
    squares = v * v
    high = squares.astype(BF16)
    low = (squares - high.astype(F32)).astype(BF16)
    row_id = lax.broadcasted_iota(jnp.int32, (width, width), 0) // HEAD_DIM
    col_id = lax.broadcasted_iota(jnp.int32, (width, width), 1) // HEAD_DIM
    average = jnp.where(row_id == col_id, 1.0 / HEAD_DIM, 0.0).astype(BF16)
    mean = jnp.dot(high, average, preferred_element_type=F32) + jnp.dot(
        low, average, preferred_element_type=F32
    )
    normed = (v * lax.rsqrt(mean + NORM_EPS) * gain_ref[...]).astype(BF16)
    part = jnp.dot(normed, w_ref[...], preferred_element_type=F32)

    @pl.when(group == 0)
    def _():
        acc_ref[...] = part

    @pl.when(group > 0)
    def _():
        acc_ref[...] += part

    @pl.when(group == pl.num_programs(0) - 1)
    def _():
        out_ref[...] = acc_ref[...].astype(BF16)


def body(
    stream_x, stream_b, stream_c, gate_z, step_raw,
    conv_x, conv_b, conv_c, decay_log, norm_gain, w_out,
):
    ranks = lax.axis_size("sp")
    me = lax.axis_index("sp")
    x, b, c, z, raw = (v[0] for v in (stream_x, stream_b, stream_c, gate_z, step_raw))
    tokens, inner_width = x.shape
    groups = b.shape[1] // STATE
    heads = raw.shape[1]
    width = RATIO * HEAD_DIM
    own = heads // ranks

    dt = jax.nn.softplus(jnp.transpose(raw).astype(F32))
    sums = jnp.sum(dt, axis=1)
    small = jnp.concatenate(
        [
            conv_x.astype(F32),
            jnp.broadcast_to(decay_log[:, None], (own, 128)),
            jnp.pad(sums, (0, 128 - heads))[None],
            jnp.zeros((1, 128), F32),
        ]
    )
    shared = lax.all_to_all(
        jnp.broadcast_to(small[None], (ranks,) + small.shape), "sp", 0, 0, tiled=True
    )
    ends = jnp.concatenate([x[tokens - HALO :], b[tokens - HALO :], c[tokens - HALO :]], axis=1)
    halo = lax.ppermute(ends, "sp", [(i, i + 1) for i in range(ranks - 1)])
    w_full = lax.all_gather(w_out, "dp", axis=0, tiled=True)

    dt_group = dt.reshape(groups, RATIO, tokens)
    xb, bb = inner_width // STATE, groups
    state, xin, bin_, cum = pl.pallas_call(
        state_kernel,
        grid=(groups,),
        in_specs=[
            pl.BlockSpec((tokens, width), lambda g: (0, g)),
            pl.BlockSpec((tokens, STATE), lambda g: (0, g)),
            pl.BlockSpec((HALO, width), lambda g: (0, g)),
            pl.BlockSpec((HALO, STATE), lambda g: (0, xb + g)),
            pl.BlockSpec((2, 8, 128), lambda g: (g, 0, 0)),
            pl.BlockSpec((4, STATE), lambda g: (0, g)),
            pl.BlockSpec((1, RATIO, tokens), lambda g: (g, 0, 0)),
        ],
        out_specs=[
            pl.BlockSpec((width, STATE), lambda g: (g, 0)),
            pl.BlockSpec((tokens, width), lambda g: (0, g)),
            pl.BlockSpec((tokens, STATE), lambda g: (0, g)),
            pl.BlockSpec((1, 2 * RATIO, tokens), lambda g: (g, 0, 0)),
        ],
        out_shape=[
            jax.ShapeDtypeStruct((inner_width, STATE), BF16),
            jax.ShapeDtypeStruct((tokens, inner_width), BF16),
            jax.ShapeDtypeStruct((tokens, groups * STATE), BF16),
            jax.ShapeDtypeStruct((groups, 2 * RATIO, tokens), F32),
        ],
        scratch_shapes=[
            pltpu.VMEM((HALO + tokens, width), F32),
            pltpu.VMEM((HALO + tokens, STATE), F32),
        ],
        cost_estimate=pl.CostEstimate(
            flops=4_000_000_000, bytes_accessed=2_000_000, transcendentals=400_000
        ),
        name="state",
    )(x, b, halo, halo, shared, conv_b, dt_group)

    local = lax.all_to_all(
        state.reshape(ranks, inner_width // ranks, STATE), "sp", 0, 0, tiled=True
    )

    cin, inner = pl.pallas_call(
        inner_kernel,
        grid=(groups,),
        in_specs=[
            pl.BlockSpec((tokens, STATE), lambda g: (0, g)),
            pl.BlockSpec((HALO, STATE), lambda g: (0, xb + bb + g)),
            pl.BlockSpec((4, STATE), lambda g: (0, g)),
            pl.BlockSpec((tokens, STATE), lambda g: (0, g)),
            pl.BlockSpec((tokens, width), lambda g: (0, g)),
            pl.BlockSpec((1, 2 * RATIO, tokens), lambda g: (g, 0, 0)),
        ],
        out_specs=[
            pl.BlockSpec((tokens, STATE), lambda g: (0, g)),
            pl.BlockSpec((tokens, width), lambda g: (0, g)),
        ],
        out_shape=[
            jax.ShapeDtypeStruct((tokens, groups * STATE), BF16),
            jax.ShapeDtypeStruct((tokens, inner_width), F32),
        ],
        scratch_shapes=[pltpu.VMEM((HALO + tokens, STATE), F32)],
        cost_estimate=pl.CostEstimate(
            flops=4_000_000_000, bytes_accessed=2_000_000, transcendentals=700_000
        ),
        name="inner",
    )(c, halo, conv_c, bin_, xin, cum)

    own_sums = lax.dynamic_slice_in_dim(shared[:, 6, :], me * own, own, 1)
    decay = jnp.exp(own_sums * -jnp.exp(decay_log)[None, :])
    entering = pl.pallas_call(
        scan_kernel,
        in_specs=[
            pl.BlockSpec(memory_space=pltpu.SMEM),
            pl.BlockSpec(memory_space=pltpu.VMEM),
        ],
        out_specs=pl.BlockSpec(memory_space=pltpu.VMEM),
        out_shape=jax.ShapeDtypeStruct(local.shape, BF16),
        cost_estimate=pl.CostEstimate(
            flops=1_000_000_000, bytes_accessed=1_000_000, transcendentals=0
        ),
        name="scan",
    )(decay, local)
    entering = lax.all_to_all(entering, "sp", 0, 0, tiled=True).reshape(inner_width, STATE)

    mixed = pl.pallas_call(
        out_kernel,
        grid=(groups,),
        in_specs=[
            pl.BlockSpec((width, STATE), lambda g: (g, 0)),
            pl.BlockSpec((tokens, STATE), lambda g: (0, g)),
            pl.BlockSpec((tokens, width), lambda g: (0, g)),
            pl.BlockSpec((1, 2 * RATIO, tokens), lambda g: (g, 0, 0)),
            pl.BlockSpec((tokens, width), lambda g: (0, g)),
            pl.BlockSpec((1, width), lambda g: (0, g)),
            pl.BlockSpec((width, w_full.shape[1]), lambda g: (g, 0)),
        ],
        out_specs=pl.BlockSpec((tokens, w_full.shape[1]), lambda g: (0, 0)),
        out_shape=jax.ShapeDtypeStruct((tokens, w_full.shape[1]), BF16),
        scratch_shapes=[pltpu.VMEM((tokens, w_full.shape[1]), F32)],
        cost_estimate=pl.CostEstimate(
            flops=4_000_000_000, bytes_accessed=10_000_000, transcendentals=300_000
        ),
        name="project",
    )(entering, cin, inner, cum, z, norm_gain[None], w_full)
    return mixed[None]


def solution(mesh):
    placed = (
        P("dp", "sp", None),
        P("dp", "sp", None),
        P("dp", "sp", None),
        P("dp", "sp", None),
        P("dp", "sp", None),
        P(None, "sp"),
        P(),
        P(),
        P("sp"),
        P(),
        P("dp", None),
    )
    return jax.shard_map(
        body, mesh=mesh, in_specs=placed, out_specs=P("dp", "sp", None), check_vma=False
    )
```

```python
import jax
import jax.numpy as jnp
from jax import lax
from jax.experimental import pallas as pl
from jax.experimental.pallas import tpu as pltpu
from jax.sharding import PartitionSpec as P

HEAD_DIM = 64
STATE = 128
RATIO = 4
WIDTH = RATIO * HEAD_DIM
NORM_EPS = 1.0
HIGHEST = lax.Precision.HIGHEST
F32 = jnp.float32
BF16 = jnp.bfloat16
HALO = 4
PAD = 8
CHUNKS = 4
MIB = 1 << 20


def silu(u):
    half = 0.5 * u
    return half + half * jnp.tanh(half)


def conv_silu(pad_ref, halo, value, taps):
    rows = value.shape[0]
    pad_ref[PAD - HALO : PAD, :] = halo.astype(F32)
    pad_ref[PAD : PAD + rows, :] = value.astype(F32)
    total = taps[3:4, :] * pad_ref[PAD : PAD + rows, :]
    for back in range(1, 4):
        total = total + taps[3 - back : 4 - back, :] * pad_ref[PAD - back : PAD - back + rows, :]
    return silu(total)


def per_head(columns, first):
    tokens = columns.shape[0]
    lane = lax.broadcasted_iota(jnp.int32, (tokens, 128), 1)
    left = jnp.broadcast_to(columns[:, first : first + 1], (tokens, 128))
    right = jnp.broadcast_to(columns[:, first + 1 : first + 2], (tokens, 128))
    return jnp.where(lane < HEAD_DIM, left, right)


def share_kernel(decay_ref, raw_ref, taps_ref, x_ref, b_ref, c_ref, small_ref, ends_ref, dt_ref):
    tokens, heads = raw_ref.shape
    ranks = small_ref.shape[0]
    raw = jnp.transpose(raw_ref[...].astype(F32))
    dt = jnp.maximum(raw, 0.0) + jnp.log1p(jnp.exp(-jnp.abs(raw)))
    src = lax.broadcasted_iota(jnp.int32, (tokens, tokens), 0)
    dst = lax.broadcasted_iota(jnp.int32, (tokens, tokens), 1)
    upper = (src <= dst).astype(F32)
    prefix = jnp.dot(dt, upper, precision=HIGHEST, preferred_element_type=F32)
    for group in range(heads // RATIO):
        rows = slice(group * RATIO, (group + 1) * RATIO)
        dt_ref[group, 0:RATIO, :] = prefix[rows]
        dt_ref[group, RATIO:, :] = dt[rows]
    ones = jnp.ones((8, tokens), F32)
    sums = lax.dot_general(
        ones, dt, (((1,), (1,)), ((), ())), precision=HIGHEST, preferred_element_type=F32
    )
    small = jnp.concatenate(
        [
            taps_ref[...].astype(F32),
            jnp.full((1, 128), decay_ref[0], F32),
            jnp.full((1, 128), decay_ref[1], F32),
            jnp.concatenate([sums[0:1], jnp.zeros((1, 128 - heads), F32)], axis=1),
            jnp.zeros((1, 128), F32),
        ],
        axis=0,
    )
    for rank in range(ranks):
        small_ref[rank] = small
    left = 0
    for ref in (x_ref, b_ref, c_ref):
        cols = ref.shape[1]
        ends_ref[:, left : left + cols] = ref[ref.shape[0] - HALO :, :]
        left += cols


def state_kernel(
    x_ref, b_ref, hx_ref, hb_ref, shared_ref, tb_ref, dt_ref,
    state_ref, xin_ref, bin_ref, cum_ref, padx_ref, padb_ref,
):
    tokens = x_ref.shape[0]
    for k in range(dt_ref.shape[0]):
        wide = slice(k * WIDTH, (k + 1) * WIDTH)
        thin = slice(k * STATE, (k + 1) * STATE)
        rows = dt_ref[k]
        logs = jnp.concatenate(
            [shared_ref[2 * k, 4:6, :], shared_ref[2 * k + 1, 4:6, :]], axis=0
        )
        cum = -jnp.exp(logs) * rows[0:RATIO]
        dt = rows[RATIO:]
        cum_ref[k] = jnp.concatenate([cum, dt], axis=0)
        tail = jnp.exp(cum[:, tokens - 1 : tokens] - cum) * dt
        columns = jnp.transpose(jnp.concatenate([tail, tail], axis=0))
        taps_x = jnp.concatenate([shared_ref[2 * k, 0:4], shared_ref[2 * k + 1, 0:4]], axis=1)
        xin = conv_silu(padx_ref.at[k], hx_ref[:, wide], x_ref[:, wide], taps_x)
        xin = xin.astype(BF16)
        bin_ = conv_silu(padb_ref.at[k], hb_ref[:, thin], b_ref[:, thin], tb_ref[:, thin].astype(F32))
        bin_ = bin_.astype(BF16)
        xin_ref[:, wide] = xin
        bin_ref[:, thin] = bin_
        scale = jnp.concatenate([per_head(columns, 0), per_head(columns, 2)], axis=1)
        scaled = (xin.astype(F32) * scale).astype(BF16)
        state = lax.dot_general(
            bin_, scaled, (((0,), (0,)), ((), ())), preferred_element_type=F32
        ).astype(BF16)
        state_ref[2 * k] = state[:, :STATE]
        state_ref[2 * k + 1] = state[:, STATE:]


def inner_kernel(c_ref, hc_ref, tc_ref, bin_ref, xin_ref, cum_ref, cin_ref, inner_ref, padc_ref):
    tokens = c_ref.shape[0]
    cin = conv_silu(padc_ref, hc_ref[...], c_ref[...], tc_ref[...].astype(F32)).astype(BF16)
    cin_ref[...] = cin
    scores = lax.dot_general(
        cin, bin_ref[...], (((1,), (1,)), ((), ())), preferred_element_type=F32
    )
    rows = cum_ref[0]
    columns = jnp.transpose(rows)
    row_id = lax.broadcasted_iota(jnp.int32, (tokens, tokens), 0)
    col_id = lax.broadcasted_iota(jnp.int32, (tokens, tokens), 1)
    causal = row_id >= col_id
    for head in range(RATIO):
        spread = columns[:, head : head + 1] - rows[head : head + 1, :]
        decay = jnp.exp(jnp.where(causal, spread, -jnp.inf))
        weights = (scores * decay * rows[RATIO + head : RATIO + head + 1, :]).astype(BF16)
        cols = slice(head * HEAD_DIM, (head + 1) * HEAD_DIM)
        inner_ref[:, cols] = jnp.dot(weights, xin_ref[:, cols], preferred_element_type=F32)


def scan_kernel(decay_ref, local_ref, out_ref):
    count = local_ref.shape[0]
    for part in range(STATE // 32):
        rows = slice(part * 32, (part + 1) * 32)
        entering = jnp.zeros((32, 2 * HEAD_DIM), F32)
        for step in range(count):
            out_ref[step, rows, :] = entering.astype(BF16)
            if step + 1 < count:
                entering = entering * decay_ref[step : step + 1, :] + local_ref[
                    step, rows, :
                ].astype(F32)


def out_kernel(
    ent_ref, cin_ref, inner_ref, cum_ref, z_ref, gain_ref, w_ref, out_ref, normed_ref, held_ref, sems
):
    chunk = w_ref.shape[1] // CHUNKS
    copies = []
    for k in range(CHUNKS):
        cols = slice(k * chunk, (k + 1) * chunk)
        copies.append(
            pltpu.make_async_copy(w_ref.at[:, cols], held_ref.at[:, cols], sems.at[k])
        )
        copies[k].start()
    row_id = lax.broadcasted_iota(jnp.int32, (STATE, STATE), 0) // HEAD_DIM
    col_id = lax.broadcasted_iota(jnp.int32, (STATE, STATE), 1) // HEAD_DIM
    average = jnp.where(row_id == col_id, 1.0 / HEAD_DIM, 0.0).astype(BF16)
    for group in range(cum_ref.shape[0]):
        columns = jnp.transpose(jnp.exp(cum_ref[group]))
        cin = cin_ref[:, group * STATE : (group + 1) * STATE]
        for half in range(2):
            pair = 2 * group + half
            cols = slice(pair * STATE, (pair + 1) * STATE)
            carried = jnp.dot(cin, ent_ref[pair], preferred_element_type=F32)
            core = inner_ref[:, cols] + carried * per_head(columns, 2 * half)
            v = core.astype(BF16).astype(F32) * silu(z_ref[:, cols].astype(F32))
            squares = v * v
            high = squares.astype(BF16)
            low = (squares - high.astype(F32)).astype(BF16)
            mean = jnp.dot(high, average, preferred_element_type=F32) + jnp.dot(
                low, average, preferred_element_type=F32
            )
            normed = v * lax.rsqrt(mean + NORM_EPS) * gain_ref[:, cols]
            normed_ref[:, cols] = normed.astype(BF16)
    for k in range(CHUNKS):
        cols = slice(k * chunk, (k + 1) * chunk)
        copies[k].wait()
        out_ref[:, cols] = jnp.dot(
            normed_ref[...], held_ref[:, cols], preferred_element_type=F32
        ).astype(BF16)


def vmem():
    return pl.BlockSpec(memory_space=pltpu.VMEM)


def cost(flops, moved, special):
    return pl.CostEstimate(flops=flops, bytes_accessed=moved, transcendentals=special)


def body(
    stream_x, stream_b, stream_c, gate_z, step_raw,
    conv_x, conv_b, conv_c, decay_log, norm_gain, w_out,
):
    ranks = lax.axis_size("sp")
    me = lax.axis_index("sp")
    x, b, c, z, raw = (v[0] for v in (stream_x, stream_b, stream_c, gate_z, step_raw))
    tokens, inner_width = x.shape
    groups = b.shape[1] // STATE
    heads = raw.shape[1]
    own = heads // ranks
    thin = groups * STATE
    last = tokens // 8 - 1

    w_full = lax.all_gather(w_out, "dp", axis=0, tiled=True)

    small, ends, dt = pl.pallas_call(
        share_kernel,
        grid=(1,),
        in_specs=[
            pl.BlockSpec(memory_space=pltpu.SMEM),
            pl.BlockSpec((tokens, heads), lambda i: (0, 0)),
            pl.BlockSpec((4, 128), lambda i: (0, 0)),
            pl.BlockSpec((8, inner_width), lambda i: (last, 0)),
            pl.BlockSpec((8, thin), lambda i: (last, 0)),
            pl.BlockSpec((8, thin), lambda i: (last, 0)),
        ],
        out_specs=[
            pl.BlockSpec((ranks, 8, 128), lambda i: (0, 0, 0)),
            pl.BlockSpec((HALO, inner_width + 2 * thin), lambda i: (0, 0)),
            pl.BlockSpec((groups, 2 * RATIO, tokens), lambda i: (0, 0, 0)),
        ],
        out_shape=[
            jax.ShapeDtypeStruct((ranks, 8, 128), F32),
            jax.ShapeDtypeStruct((HALO, inner_width + 2 * thin), BF16),
            jax.ShapeDtypeStruct((groups, 2 * RATIO, tokens), F32),
        ],
        compiler_params=pltpu.CompilerParams(vmem_limit_bytes=8 * MIB),
        cost_estimate=cost(10_000_000, 200_000, 10_000),
        name="share",
    )(decay_log, raw, conv_x, x, b, c)
    shared = lax.all_to_all(small, "sp", 0, 0, tiled=True)
    halo = lax.ppermute(ends, "sp", [(i, i + 1) for i in range(ranks - 1)])

    xb, bb = inner_width // STATE, groups
    per = 2
    state, xin, bin_, cum = pl.pallas_call(
        state_kernel,
        grid=(groups // per,),
        in_specs=[
            pl.BlockSpec((tokens, per * WIDTH), lambda g: (0, g)),
            pl.BlockSpec((tokens, per * STATE), lambda g: (0, g)),
            pl.BlockSpec((HALO, per * WIDTH), lambda g: (0, g)),
            pl.BlockSpec((HALO, per * STATE), lambda g: (0, xb // per + g)),
            pl.BlockSpec((2 * per, 8, 128), lambda g: (g, 0, 0)),
            pl.BlockSpec((4, per * STATE), lambda g: (0, g)),
            pl.BlockSpec((per, 2 * RATIO, tokens), lambda g: (g, 0, 0)),
        ],
        out_specs=[
            pl.BlockSpec((2 * per, STATE, STATE), lambda g: (g, 0, 0)),
            pl.BlockSpec((tokens, per * WIDTH), lambda g: (0, g)),
            pl.BlockSpec((tokens, per * STATE), lambda g: (0, g)),
            pl.BlockSpec((per, 2 * RATIO, tokens), lambda g: (g, 0, 0)),
        ],
        out_shape=[
            jax.ShapeDtypeStruct((ranks, STATE, inner_width // ranks), BF16),
            jax.ShapeDtypeStruct((tokens, inner_width), BF16),
            jax.ShapeDtypeStruct((tokens, thin), BF16),
            jax.ShapeDtypeStruct((groups, 2 * RATIO, tokens), F32),
        ],
        scratch_shapes=[
            pltpu.VMEM((per, PAD + tokens, WIDTH), F32),
            pltpu.VMEM((per, PAD + tokens, STATE), F32),
        ],
        compiler_params=pltpu.CompilerParams(vmem_limit_bytes=16 * MIB),
        cost_estimate=cost(4_000_000_000, 2_000_000, 400_000),
        name="state",
    )(x, b, halo, halo, shared, conv_b, dt)

    local = lax.all_to_all(state, "sp", 0, 0, tiled=True)

    cin, inner = pl.pallas_call(
        inner_kernel,
        grid=(groups,),
        in_specs=[
            pl.BlockSpec((tokens, STATE), lambda g: (0, g)),
            pl.BlockSpec((HALO, STATE), lambda g: (0, xb + bb + g)),
            pl.BlockSpec((4, STATE), lambda g: (0, g)),
            pl.BlockSpec((tokens, STATE), lambda g: (0, g)),
            pl.BlockSpec((tokens, WIDTH), lambda g: (0, g)),
            pl.BlockSpec((1, 2 * RATIO, tokens), lambda g: (g, 0, 0)),
        ],
        out_specs=[
            pl.BlockSpec((tokens, STATE), lambda g: (0, g)),
            pl.BlockSpec((tokens, WIDTH), lambda g: (0, g)),
        ],
        out_shape=[
            jax.ShapeDtypeStruct((tokens, thin), BF16),
            jax.ShapeDtypeStruct((tokens, inner_width), F32),
        ],
        scratch_shapes=[pltpu.VMEM((PAD + tokens, STATE), F32)],
        compiler_params=pltpu.CompilerParams(vmem_limit_bytes=16 * MIB),
        cost_estimate=cost(4_000_000_000, 2_000_000, 700_000),
        name="inner",
    )(c, halo, conv_c, bin_, xin, cum)

    own_sums = lax.dynamic_slice_in_dim(shared[:, 6, :], me * own, own, 1)
    decay = jnp.repeat(jnp.exp(own_sums * -jnp.exp(decay_log)[None, :]), HEAD_DIM, axis=1)
    entering = pl.pallas_call(
        scan_kernel,
        in_specs=[vmem(), vmem()],
        out_specs=vmem(),
        out_shape=jax.ShapeDtypeStruct(local.shape, BF16),
        compiler_params=pltpu.CompilerParams(vmem_limit_bytes=8 * MIB),
        cost_estimate=cost(1_000_000_000, 1_000_000, 0),
        name="scan",
    )(decay, local)
    entering = lax.all_to_all(entering, "sp", 0, 0, tiled=True)

    mixed = pl.pallas_call(
        out_kernel,
        in_specs=[vmem()] * 6 + [pl.BlockSpec(memory_space=pltpu.HBM)],
        out_specs=vmem(),
        out_shape=jax.ShapeDtypeStruct((tokens, w_full.shape[1]), BF16),
        scratch_shapes=[
            pltpu.VMEM((tokens, inner_width), BF16),
            pltpu.VMEM(w_full.shape, BF16),
            pltpu.SemaphoreType.DMA((CHUNKS,)),
        ],
        compiler_params=pltpu.CompilerParams(vmem_limit_bytes=24 * MIB),
        cost_estimate=cost(4_000_000_000, 10_000_000, 300_000),
        name="project",
    )(entering, cin, inner, cum, z, norm_gain[None], w_full)
    return mixed[None]


def solution(mesh):
    placed = (
        P("dp", "sp", None),
        P("dp", "sp", None),
        P("dp", "sp", None),
        P("dp", "sp", None),
        P("dp", "sp", None),
        P(None, "sp"),
        P(),
        P(),
        P("sp"),
        P(),
        P("dp", None),
    )
    return jax.shard_map(
        body, mesh=mesh, in_specs=placed, out_specs=P("dp", "sp", None), check_vma=False
    )
```

```python
import jax
import jax.numpy as jnp
from jax import lax
from jax.experimental import pallas as pl
from jax.experimental.pallas import tpu as pltpu
from jax.sharding import PartitionSpec as P

HEAD_DIM = 64
STATE = 128
RATIO = 4
WIDTH = RATIO * HEAD_DIM
NORM_EPS = 1.0
HIGHEST = lax.Precision.HIGHEST
F32 = jnp.float32
BF16 = jnp.bfloat16
HALO = 4
PAD = 8
MIB = 1 << 20
WHOLE = 16 * MIB
OUT_LIMIT = 20 * MIB


def silu(u):
    half = 0.5 * u
    return half + half * jnp.tanh(half)


def conv_silu(pad_ref, halo, value, taps):
    rows = value.shape[0]
    pad_ref[PAD - HALO : PAD, :] = halo.astype(F32)
    pad_ref[PAD : PAD + rows, :] = value.astype(F32)
    total = taps[3:4, :] * pad_ref[PAD : PAD + rows, :]
    for back in range(1, 4):
        total = total + taps[3 - back : 4 - back, :] * pad_ref[PAD - back : PAD - back + rows, :]
    return silu(total)


def per_head(columns, first):
    tokens = columns.shape[0]
    lane = lax.broadcasted_iota(jnp.int32, (tokens, 128), 1)
    left = jnp.broadcast_to(columns[:, first : first + 1], (tokens, 128))
    right = jnp.broadcast_to(columns[:, first + 1 : first + 2], (tokens, 128))
    return jnp.where(lane < HEAD_DIM, left, right)


def share_kernel(decay_ref, raw_ref, taps_ref, x_ref, b_ref, c_ref, small_ref, ends_ref, dt_ref):
    heads, tokens = raw_ref.shape
    ranks = small_ref.shape[0]
    raw = raw_ref[...].astype(F32)
    dt = jnp.maximum(raw, 0.0) + jnp.log1p(jnp.exp(-jnp.abs(raw)))
    src = lax.broadcasted_iota(jnp.int32, (tokens, tokens), 0)
    dst = lax.broadcasted_iota(jnp.int32, (tokens, tokens), 1)
    upper = (src <= dst).astype(F32)
    prefix = jnp.dot(dt, upper, precision=HIGHEST, preferred_element_type=F32)
    for group in range(heads // RATIO):
        rows = slice(group * RATIO, (group + 1) * RATIO)
        dt_ref[group, 0:RATIO, :] = prefix[rows]
        dt_ref[group, RATIO:, :] = dt[rows]
    ones = jnp.ones((8, tokens), F32)
    sums = lax.dot_general(
        ones, dt, (((1,), (1,)), ((), ())), precision=HIGHEST, preferred_element_type=F32
    )
    small = jnp.concatenate(
        [
            taps_ref[...].astype(F32),
            jnp.full((1, 128), decay_ref[0], F32),
            jnp.full((1, 128), decay_ref[1], F32),
            jnp.concatenate([sums[0:1], jnp.zeros((1, 128 - heads), F32)], axis=1),
            jnp.zeros((1, 128), F32),
        ],
        axis=0,
    )
    for rank in range(ranks):
        small_ref[rank] = small
    left = 0
    for ref in (x_ref, b_ref, c_ref):
        cols = ref.shape[1]
        ends_ref[:, left : left + cols] = ref[ref.shape[0] - HALO :, :]
        left += cols


def state_kernel(
    x_ref, b_ref, hx_ref, hb_ref, shared_ref, tb_ref, dt_ref,
    state_ref, xin_ref, bin_ref, cum_ref, padx_ref, padb_ref,
):
    tokens = x_ref.shape[0]
    for k in range(dt_ref.shape[0]):
        wide = slice(k * WIDTH, (k + 1) * WIDTH)
        thin = slice(k * STATE, (k + 1) * STATE)
        rows = dt_ref[k]
        logs = jnp.concatenate(
            [shared_ref[2 * k, 4:6, :], shared_ref[2 * k + 1, 4:6, :]], axis=0
        )
        cum = -jnp.exp(logs) * rows[0:RATIO]
        dt = rows[RATIO:]
        cum_ref[k] = jnp.concatenate([cum, dt], axis=0)
        tail = jnp.exp(cum[:, tokens - 1 : tokens] - cum) * dt
        columns = jnp.transpose(jnp.concatenate([tail, tail], axis=0))
        taps_x = jnp.concatenate([shared_ref[2 * k, 0:4], shared_ref[2 * k + 1, 0:4]], axis=1)
        xin = conv_silu(padx_ref.at[k], hx_ref[:, wide], x_ref[:, wide], taps_x)
        xin = xin.astype(BF16)
        bin_ = conv_silu(padb_ref.at[k], hb_ref[:, thin], b_ref[:, thin], tb_ref[:, thin].astype(F32))
        bin_ = bin_.astype(BF16)
        xin_ref[:, wide] = xin
        bin_ref[:, thin] = bin_
        scale = jnp.concatenate([per_head(columns, 0), per_head(columns, 2)], axis=1)
        scaled = (xin.astype(F32) * scale).astype(BF16)
        state = lax.dot_general(
            bin_, scaled, (((0,), (0,)), ((), ())), preferred_element_type=F32
        ).astype(BF16)
        state_ref[2 * k] = state[:, :STATE]
        state_ref[2 * k + 1] = state[:, STATE:]


def inner_kernel(c_ref, hc_ref, tc_ref, bin_ref, xin_ref, cum_ref, cin_ref, inner_ref, padc_ref):
    tokens = c_ref.shape[0]
    cin = conv_silu(padc_ref, hc_ref[...], c_ref[...], tc_ref[...].astype(F32)).astype(BF16)
    cin_ref[...] = cin
    scores = lax.dot_general(
        cin, bin_ref[...], (((1,), (1,)), ((), ())), preferred_element_type=F32
    )
    rows = cum_ref[0]
    columns = jnp.transpose(rows)
    row_id = lax.broadcasted_iota(jnp.int32, (tokens, tokens), 0)
    col_id = lax.broadcasted_iota(jnp.int32, (tokens, tokens), 1)
    causal = row_id >= col_id
    for head in range(RATIO):
        spread = columns[:, head : head + 1] - rows[head : head + 1, :]
        decay = jnp.exp(jnp.where(causal, spread, -jnp.inf))
        weights = (scores * decay * rows[RATIO + head : RATIO + head + 1, :]).astype(BF16)
        cols = slice(head * HEAD_DIM, (head + 1) * HEAD_DIM)
        inner_ref[:, cols] = jnp.dot(weights, xin_ref[:, cols], preferred_element_type=F32)


def scan_kernel(decay_ref, shared_ref, local_ref, out_ref):
    count = local_ref.shape[0]
    me = lax.axis_index("sp")
    sums = shared_ref[:, 6, :]
    lane = lax.broadcasted_iota(jnp.int32, sums.shape, 1)
    ends = []
    for head in range(2):
        mine = jnp.sum(jnp.where(lane == 2 * me + head, sums, 0.0), axis=1, keepdims=True)
        rate = jnp.exp(jnp.full(sums.shape, decay_ref[head], F32))
        ends.append(jnp.exp(-rate * mine))
    decay = jnp.where(lane < HEAD_DIM, ends[0], ends[1])
    for part in range(STATE // 32):
        rows = slice(part * 32, (part + 1) * 32)
        entering = jnp.zeros((32, 2 * HEAD_DIM), F32)
        for step in range(count):
            out_ref[step, rows, :] = entering.astype(BF16)
            if step + 1 < count:
                entering = entering * decay[step : step + 1, :] + local_ref[
                    step, rows, :
                ].astype(F32)


def out_kernel(
    ent_ref, cin_ref, inner_ref, cum_ref, z_ref, gain_ref,
    m0_ref, m1_ref, m2_ref, m3_ref, o0_ref, o1_ref, o2_ref, o3_ref,
    out_ref, normed_ref, ordered_ref, held_ref, acc_ref, sems,
):
    rank = lax.axis_index("dp")
    y, x, core = rank // 8, lax.rem(rank // 2, 4), lax.rem(rank, 2)
    pieces = (m0_ref, m1_ref, m2_ref, m3_ref, o0_ref, o1_ref, o2_ref, o3_ref)
    deep = m0_ref.shape[0]
    copies = [
        pltpu.make_async_copy(ref, held_ref.at[k * deep : (k + 1) * deep, :], sems.at[k])
        for k, ref in enumerate(pieces)
    ]
    for copy in copies:
        copy.start()
    row_id = lax.broadcasted_iota(jnp.int32, (STATE, STATE), 0) // HEAD_DIM
    col_id = lax.broadcasted_iota(jnp.int32, (STATE, STATE), 1) // HEAD_DIM
    average = jnp.where(row_id == col_id, 1.0 / HEAD_DIM, 0.0).astype(BF16)
    for group in range(cum_ref.shape[0]):
        columns = jnp.transpose(jnp.exp(cum_ref[group]))
        cin = cin_ref[:, group * STATE : (group + 1) * STATE]
        for half in range(2):
            pair = 2 * group + half
            cols = slice(pair * STATE, (pair + 1) * STATE)
            carried = jnp.dot(cin, ent_ref[pair], preferred_element_type=F32)
            core_out = inner_ref[:, cols] + carried * per_head(columns, 2 * half)
            v = core_out.astype(BF16).astype(F32) * silu(z_ref[:, cols].astype(F32))
            squares = v * v
            high = squares.astype(BF16)
            low = (squares - high.astype(F32)).astype(BF16)
            mean = jnp.dot(high, average, preferred_element_type=F32) + jnp.dot(
                low, average, preferred_element_type=F32
            )
            normed_ref[pair] = v * lax.rsqrt(mean + NORM_EPS) * gain_ref[:, cols]
    tokens = out_ref.shape[0]
    lane = lax.broadcasted_iota(jnp.int32, (tokens, STATE), 1)

    def chip(side, position):
        major, minor = position // 4, position % 4
        ry = jnp.where(side == 0, major, minor)
        rx = jnp.where(side == 0, minor, major)
        return lax.rem(y + 4 - ry, 4) * 4 + lax.rem(x + 4 - rx, 4)

    for half, side in enumerate((core, 1 - core)):
        for k in range(8):
            left = normed_ref[chip(side, 2 * k)]
            right = normed_ref[chip(side, 2 * k + 1)]
            turned = pltpu.roll(jnp.where(side == 0, right, left), HEAD_DIM, 1)
            left = jnp.where(side == 0, left, turned)
            right = jnp.where(side == 0, turned, right)
            first = (half * 8 + k) * STATE
            ordered_ref[:, first : first + STATE] = jnp.where(
                lane < HEAD_DIM, left, right
            ).astype(BF16)
    chunk = 512
    stages = 4
    depth = held_ref.shape[0] // stages
    for stage in range(stages):
        for copy in copies[stage * 8 // stages : (stage + 1) * 8 // stages]:
            copy.wait()
        rows = slice(stage * depth, (stage + 1) * depth)
        for first in range(0, out_ref.shape[1], chunk):
            cols = slice(first, first + chunk)
            part = jnp.dot(
                ordered_ref[:, rows], held_ref[rows, cols], preferred_element_type=F32
            )
            if stage:
                part = part + acc_ref[:, cols]
            if stage < stages - 1:
                acc_ref[:, cols] = part
            else:
                out_ref[:, cols] = part.astype(BF16)


def vmem():
    return pl.BlockSpec(memory_space=pltpu.VMEM)


def in_hbm(*values):
    return [pltpu.with_memory_space_constraint(v, pltpu.HBM) for v in values]


def cost(flops, moved, special):
    return pl.CostEstimate(flops=flops, bytes_accessed=moved, transcendentals=special)


def first_step(y, x, core, d):
    return (y, x + d, core) if core == 0 else (y + d, x, core)


def second_step(y, x, core, d):
    return (y + d, x, core) if core == 0 else (y, x + d, core)


def swap_step(y, x, core, d):
    return y, x, 1 - core


def torus(step, d):
    pairs = []
    for rank in range(32):
        y, x, core = step(rank // 8, rank // 2 % 4, rank % 2, d)
        pairs.append((rank, ((y % 4) * 4 + x % 4) * 2 + core))
    return pairs


def body(
    stream_x, stream_b, stream_c, gate_z, step_raw,
    conv_x, conv_b, conv_c, decay_log, norm_gain, w_out,
):
    ranks = lax.axis_size("sp")
    x, b, c, z, raw = (v[0] for v in (stream_x, stream_b, stream_c, gate_z, step_raw))
    tokens, inner_width = x.shape
    groups = b.shape[1] // STATE
    heads = raw.shape[1]
    thin = groups * STATE
    last = tokens // 8 - 1

    near = [lax.ppermute(w_out, "dp", torus(first_step, d)) for d in (1, 2, 3)]
    row = jnp.concatenate([w_out] + near)
    mine = [row] + [lax.ppermute(row, "dp", torus(second_step, d)) for d in (1, 2, 3)]
    other = [lax.ppermute(v, "dp", torus(swap_step, 0)) for v in mine]

    small, ends, dt = pl.pallas_call(
        share_kernel,
        grid=(1,),
        in_specs=[
            pl.BlockSpec(memory_space=pltpu.SMEM),
            pl.BlockSpec((heads, tokens), lambda i: (0, 0)),
            pl.BlockSpec((4, 128), lambda i: (0, 0)),
            pl.BlockSpec((8, inner_width), lambda i: (last, 0)),
            pl.BlockSpec((8, thin), lambda i: (last, 0)),
            pl.BlockSpec((8, thin), lambda i: (last, 0)),
        ],
        out_specs=[
            pl.BlockSpec((ranks, 8, 128), lambda i: (0, 0, 0)),
            pl.BlockSpec((HALO, inner_width + 2 * thin), lambda i: (0, 0)),
            pl.BlockSpec((groups, 2 * RATIO, tokens), lambda i: (0, 0, 0)),
        ],
        out_shape=[
            jax.ShapeDtypeStruct((ranks, 8, 128), F32),
            jax.ShapeDtypeStruct((HALO, inner_width + 2 * thin), BF16),
            jax.ShapeDtypeStruct((groups, 2 * RATIO, tokens), F32),
        ],
        compiler_params=pltpu.CompilerParams(vmem_limit_bytes=WHOLE),
        cost_estimate=cost(10_000_000, 200_000, 10_000),
        name="share",
    )(decay_log, jnp.transpose(raw), conv_x, *in_hbm(x, b, c))
    shared = lax.all_to_all(small, "sp", 0, 0, tiled=True)
    halo = lax.ppermute(ends, "sp", [(i, i + 1) for i in range(ranks - 1)])

    xb, bb = inner_width // STATE, groups
    per = 2
    state, xin, bin_, cum = pl.pallas_call(
        state_kernel,
        grid=(groups // per,),
        in_specs=[
            pl.BlockSpec((tokens, per * WIDTH), lambda g: (0, g)),
            pl.BlockSpec((tokens, per * STATE), lambda g: (0, g)),
            pl.BlockSpec((HALO, per * WIDTH), lambda g: (0, g)),
            pl.BlockSpec((HALO, per * STATE), lambda g: (0, xb // per + g)),
            pl.BlockSpec((2 * per, 8, 128), lambda g: (g, 0, 0)),
            pl.BlockSpec((4, per * STATE), lambda g: (0, g)),
            pl.BlockSpec((per, 2 * RATIO, tokens), lambda g: (g, 0, 0)),
        ],
        out_specs=[
            pl.BlockSpec((2 * per, STATE, STATE), lambda g: (g, 0, 0)),
            pl.BlockSpec((tokens, per * WIDTH), lambda g: (0, g)),
            pl.BlockSpec((tokens, per * STATE), lambda g: (0, g)),
            pl.BlockSpec((per, 2 * RATIO, tokens), lambda g: (g, 0, 0)),
        ],
        out_shape=[
            jax.ShapeDtypeStruct((ranks, STATE, inner_width // ranks), BF16),
            jax.ShapeDtypeStruct((tokens, inner_width), BF16),
            jax.ShapeDtypeStruct((tokens, thin), BF16),
            jax.ShapeDtypeStruct((groups, 2 * RATIO, tokens), F32),
        ],
        scratch_shapes=[
            pltpu.VMEM((per, PAD + tokens, WIDTH), F32),
            pltpu.VMEM((per, PAD + tokens, STATE), F32),
        ],
        compiler_params=pltpu.CompilerParams(vmem_limit_bytes=WHOLE),
        cost_estimate=cost(4_000_000_000, 2_000_000, 400_000),
        name="state",
    )(*in_hbm(x, b), halo, halo, shared, conv_b, dt)

    local = lax.all_to_all(state, "sp", 0, 0, tiled=True)

    cin, inner = pl.pallas_call(
        inner_kernel,
        grid=(groups,),
        in_specs=[
            pl.BlockSpec((tokens, STATE), lambda g: (0, g)),
            pl.BlockSpec((HALO, STATE), lambda g: (0, xb + bb + g)),
            pl.BlockSpec((4, STATE), lambda g: (0, g)),
            pl.BlockSpec((tokens, STATE), lambda g: (0, g)),
            pl.BlockSpec((tokens, WIDTH), lambda g: (0, g)),
            pl.BlockSpec((1, 2 * RATIO, tokens), lambda g: (g, 0, 0)),
        ],
        out_specs=[
            pl.BlockSpec((tokens, STATE), lambda g: (0, g)),
            pl.BlockSpec((tokens, WIDTH), lambda g: (0, g)),
        ],
        out_shape=[
            jax.ShapeDtypeStruct((tokens, thin), BF16),
            jax.ShapeDtypeStruct((tokens, inner_width), F32),
        ],
        scratch_shapes=[pltpu.VMEM((PAD + tokens, STATE), F32)],
        compiler_params=pltpu.CompilerParams(vmem_limit_bytes=16 * MIB),
        cost_estimate=cost(4_000_000_000, 2_000_000, 700_000),
        name="inner",
    )(c, halo, conv_c, bin_, xin, cum)

    entering = pl.pallas_call(
        scan_kernel,
        in_specs=[pl.BlockSpec(memory_space=pltpu.SMEM), vmem(), vmem()],
        out_specs=vmem(),
        out_shape=jax.ShapeDtypeStruct(local.shape, BF16),
        compiler_params=pltpu.CompilerParams(vmem_limit_bytes=8 * MIB),
        cost_estimate=cost(1_000_000_000, 1_000_000, 0),
        name="scan",
    )(decay_log, shared, local)
    entering = lax.all_to_all(entering, "sp", 0, 0, tiled=True)

    mixed = pl.pallas_call(
        out_kernel,
        in_specs=[vmem()] * 6 + [pl.BlockSpec(memory_space=pltpu.HBM)] * 8,
        out_specs=vmem(),
        out_shape=jax.ShapeDtypeStruct((tokens, w_out.shape[1]), BF16),
        scratch_shapes=[
            pltpu.VMEM((inner_width // STATE, tokens, STATE), F32),
            pltpu.VMEM((tokens, inner_width), BF16),
            pltpu.VMEM((inner_width, w_out.shape[1]), BF16),
            pltpu.VMEM((tokens, w_out.shape[1]), F32),
            pltpu.SemaphoreType.DMA((8,)),
        ],
        compiler_params=pltpu.CompilerParams(vmem_limit_bytes=OUT_LIMIT),
        cost_estimate=cost(4_000_000_000, 10_000_000, 300_000),
        name="project",
    )(entering, cin, inner, cum, z, norm_gain[None], *in_hbm(*mine, *other))
    return mixed[None]


def solution(mesh):
    placed = (
        P("dp", "sp", None),
        P("dp", "sp", None),
        P("dp", "sp", None),
        P("dp", "sp", None),
        P("dp", "sp", None),
        P(None, "sp"),
        P(),
        P(),
        P("sp"),
        P(),
        P("dp", None),
    )
    return jax.shard_map(
        body, mesh=mesh, in_specs=placed, out_specs=P("dp", "sp", None), check_vma=False
    )
```

```python
import jax
import jax.numpy as jnp
from jax import lax
from jax.experimental import pallas as pl
from jax.experimental.pallas import tpu as pltpu
from jax.sharding import PartitionSpec as P


HEAD_DIM = 64
STATE = 128
RATIO = 4
WIDTH = RATIO * HEAD_DIM
NORM_EPS = 1.0
HIGHEST = lax.Precision.HIGHEST
F32 = jnp.float32
BF16 = jnp.bfloat16
HALO = 4
EXTRA = 8
REACH = 3
COMMON = 16
PAD = 8
MIB = 1 << 20
OUT_LIMIT = 20 * MIB


def silu(u):
    half = 0.5 * u
    return half + half * jnp.tanh(half)


def lanes(first, size):
    return pl.ds(pl.multiple_of(first, STATE), size)


def conv_silu(pad_ref, halo, own, given, side, taps):
    tokens = own.shape[0]
    rows = 2 * tokens
    pad_ref[PAD - HALO : PAD, :] = halo.astype(F32)
    pad_ref[pl.ds(pl.multiple_of(PAD + side * tokens, 8), tokens), :] = own.astype(F32)
    pad_ref[pl.ds(pl.multiple_of(PAD + (1 - side) * tokens, 8), tokens), :] = given.astype(F32)
    total = taps[3:4, :] * pad_ref[PAD : PAD + rows, :]
    for back in range(1, 4):
        total = total + taps[3 - back : 4 - back, :] * pad_ref[PAD - back : PAD - back + rows, :]
    return silu(total)


def per_head(columns, first):
    tokens = columns.shape[0]
    lane = lax.broadcasted_iota(jnp.int32, (tokens, 128), 1)
    left = jnp.broadcast_to(columns[:, first : first + 1], (tokens, 128))
    right = jnp.broadcast_to(columns[:, first + 1 : first + 2], (tokens, 128))
    return jnp.where(lane < HEAD_DIM, left, right)


def head_row(values):
    lane = lax.broadcasted_iota(jnp.int32, (1, WIDTH), 1)
    row = jnp.broadcast_to(values[0:1], (1, WIDTH))
    for head in range(1, RATIO):
        row = jnp.where(
            lane >= head * HEAD_DIM, jnp.broadcast_to(values[head : head + 1], (1, WIDTH)), row
        )
    return row


def steps_of(raw):
    tokens = raw.shape[1]
    raw = raw.astype(F32)
    dt = jnp.maximum(raw, 0.0) + jnp.log1p(jnp.exp(-jnp.abs(raw)))
    src = lax.broadcasted_iota(jnp.int32, (tokens, tokens), 0)
    dst = lax.broadcasted_iota(jnp.int32, (tokens, tokens), 1)
    upper = (src <= dst).astype(F32)
    return dt, jnp.dot(dt, upper, precision=HIGHEST, preferred_element_type=F32)


def thirds(value):
    high = value.astype(BF16).astype(F32)
    rest = value - high
    middle = rest.astype(BF16).astype(F32)
    return [high, middle, rest - middle]


def share_kernel(
    decay_ref, raw_ref, taps_ref, x_ref, b_ref, c_ref,
    small_ref, dt_ref, own_ref, give_ref, own_c_ref, give_c_ref,
):
    heads, tokens = raw_ref.shape
    side = lax.rem(lax.axis_index("sp"), 2)
    other = 1 - side
    raw = raw_ref[...].astype(F32)
    left = 0
    for source in (x_ref, b_ref):
        half = source.shape[1] // 2
        own_ref[:, left : left + half] = source[:, lanes(side * half, half)]
        give_ref[0:tokens, left : left + half] = source[:, lanes(other * half, half)]
        left += half
    half = c_ref.shape[1] // 2
    own_c_ref[...] = c_ref[:, lanes(side * half, half)]
    give_c_ref[...] = c_ref[:, lanes(other * half, half)]
    theirs = jnp.where(other == 0, raw[0 : heads // 2], raw[heads // 2 :])
    per = left // tokens
    flats = []
    for first in range(0, heads // 2, per):
        held = min(per, heads // 2 - first)
        flats.append(
            jnp.concatenate(
                [theirs[first + k : first + k + 1] for k in range(held)]
                + [jnp.zeros((1, tokens), F32)] * (per - held),
                axis=1,
            )
        )
    flats.append(jnp.zeros((EXTRA - len(flats), left), F32))
    give_ref[tokens : tokens + EXTRA, :] = jnp.concatenate(flats, axis=0).astype(BF16)

    dt, prefix = steps_of(raw)
    for group in range(heads // RATIO):
        rows = slice(group * RATIO, (group + 1) * RATIO)
        dt_ref[group, 0:RATIO, :] = prefix[rows]
        dt_ref[group, RATIO:, :] = dt[rows]
    ones = jnp.ones((8, tokens), F32)
    sums = lax.dot_general(
        ones, dt, (((1,), (1,)), ((), ())), precision=HIGHEST, preferred_element_type=F32
    )
    sums = jnp.concatenate([sums[0:1], jnp.zeros((1, 128 - heads), F32)], axis=1)
    common = jnp.concatenate(
        [taps_ref[...].astype(F32)]
        + thirds(jnp.full((1, 128), decay_ref[0], F32))
        + thirds(jnp.full((1, 128), decay_ref[1], F32))
        + thirds(sums)
        + [jnp.zeros((3, 128), F32)],
        axis=0,
    ).astype(BF16)
    ends = []
    for part in range(2):
        rows = []
        tails = [ref[tokens - 8 :, :].astype(F32) for ref in (x_ref, b_ref, c_ref)]
        for token in range(8 - REACH, 8):
            for tail in tails:
                half = tail.shape[1] // 2
                for first in range(part * half, (part + 1) * half, STATE):
                    rows.append(tail[token : token + 1, first : first + STATE])
        ends.append(jnp.concatenate(rows, axis=0).astype(BF16))
    for rank in range(small_ref.shape[0]):
        small_ref[rank, 0:COMMON, :] = common
        small_ref[rank, COMMON:, :] = ends[rank % 2]


def halo_of(shared_ref, first, count):
    pair = lax.axis_index("sp") // 2
    source = jnp.maximum(2 * pair - 1, 0)
    ends = shared_ref[source, COMMON:, :].astype(F32)
    ends = jnp.where(pair == 0, 0.0, ends)
    stride = ends.shape[0] // REACH
    row_id = lax.broadcasted_iota(jnp.int32, ends.shape, 0)
    rows = [jnp.zeros((HALO - REACH, count * STATE), F32)]
    for token in range(REACH):
        picked = [
            jnp.sum(
                jnp.where(row_id == token * stride + first + k, ends, 0.0), axis=0, keepdims=True
            )
            for k in range(count)
        ]
        rows.append(jnp.concatenate(picked, axis=1))
    return jnp.concatenate(rows, axis=0)


def early_kernel(got_ref, dt_ref, steps_ref):
    side = lax.rem(lax.axis_index("sp"), 2)
    groups, _, tokens = steps_ref.shape
    flat = got_ref[...].astype(F32)
    per = flat.shape[1] // tokens
    raw = jnp.concatenate(
        [
            flat[k // per : k // per + 1, k % per * tokens : (k % per + 1) * tokens]
            for k in range(groups * RATIO)
        ],
        axis=0,
    )
    dt, prefix = steps_of(raw)
    for group in range(groups):
        rows = slice(group * RATIO, (group + 1) * RATIO)
        given = jnp.concatenate([prefix[rows], dt[rows]], axis=0)
        own = dt_ref[side * groups + group]
        steps_ref[group, 0 : 2 * RATIO, :] = jnp.where(side == 0, own, given)
        steps_ref[group, 2 * RATIO :, :] = jnp.where(side == 0, given, own)


def state_kernel(
    own_ref, own_b_ref, got_ref, got_b_ref, shared_ref, tb_ref, steps_ref,
    state_ref, first_ref, xin_ref, bin_ref, cum_ref, pad_ref, pad_b_ref,
):
    side = lax.rem(lax.axis_index("sp"), 2)
    tokens = own_ref.shape[0]
    end = tokens - 1
    per = steps_ref.shape[0]
    for k in range(per):
        wide = slice(k * WIDTH, (k + 1) * WIDTH)
        thin = slice(k * STATE, (k + 1) * STATE)
        group = per * pl.program_id(0) + k
        piece = 8 * side + 2 * group
        lower = shared_ref[piece, 0:COMMON, :].astype(F32)
        upper = shared_ref[piece + 1, 0:COMMON, :].astype(F32)
        rows = steps_ref[k]
        logs = []
        for part in (lower, upper):
            for row in (4, 7):
                logs.append(part[row : row + 1] + part[row + 1 : row + 2] + part[row + 2 : row + 3])
        rate = jnp.exp(jnp.concatenate(logs, axis=0))
        cums, tails = [], []
        for block in range(2):
            prefix = rows[8 * block : 8 * block + RATIO]
            dt = rows[8 * block + RATIO : 8 * block + 2 * RATIO]
            cum = -rate * prefix
            cums += [cum, dt]
            tails.append(jnp.exp(cum[:, end : end + 1] - cum) * dt)
        cum_ref[k] = jnp.concatenate(cums, axis=0)
        columns = jnp.transpose(jnp.concatenate(tails, axis=0))
        xin = conv_silu(
            pad_ref.at[k],
            halo_of(shared_ref, 2 * group, 2),
            own_ref[:, wide],
            got_ref[0:tokens, wide],
            side,
            jnp.concatenate([lower[0:4], upper[0:4]], axis=1),
        ).astype(BF16)
        bin_ = conv_silu(
            pad_b_ref.at[k],
            halo_of(shared_ref, 8 + group, 1),
            own_b_ref[:, thin],
            got_b_ref[0:tokens, thin],
            side,
            tb_ref[:, lanes((side * 4 + group) * STATE, STATE)].astype(F32),
        ).astype(BF16)
        bin_ref[:, thin] = bin_
        xin_ref[:, wide] = xin
        states = []
        for block in range(2):
            part = slice(block * tokens, (block + 1) * tokens)
            scale = jnp.concatenate(
                [per_head(columns, 4 * block), per_head(columns, 4 * block + 2)], axis=1
            )
            scaled = (xin[part].astype(F32) * scale).astype(BF16)
            states.append(
                lax.dot_general(
                    bin_[part],
                    scaled,
                    (((0,), (0,)), ((), ())),
                    preferred_element_type=F32,
                )
            )
        both = (states[1] + states[0] * head_row(jnp.exp(cums[2][:, end : end + 1]))).astype(BF16)
        for half in range(2):
            cols = slice(half * STATE, (half + 1) * STATE)
            first_ref[2 * k + half] = states[0][:, cols]
            for part in range(2):
                state_ref[4 * k + 2 * half + part] = both[
                    part * HEAD_DIM : (part + 1) * HEAD_DIM, cols
                ]


def inner_kernel(
    own_ref, got_ref, shared_ref, tc_ref, bin_ref, xin_ref, cum_ref,
    cin_ref, inner_ref, pad_ref,
):
    side = lax.rem(lax.axis_index("sp"), 2)
    group = pl.program_id(0)
    groups = pl.num_programs(0)
    tokens = own_ref.shape[0]
    cin = conv_silu(
        pad_ref,
        halo_of(shared_ref, 12 + group, 1),
        own_ref[...],
        got_ref[...],
        side,
        tc_ref[:, lanes((side * groups + group) * STATE, STATE)].astype(F32),
    ).astype(BF16)
    cin_ref[...] = cin
    row_id = lax.broadcasted_iota(jnp.int32, (tokens, tokens), 0)
    col_id = lax.broadcasted_iota(jnp.int32, (tokens, tokens), 1)
    causal = row_id >= col_id
    for block in range(2):
        part = slice(block * tokens, (block + 1) * tokens)
        scores = lax.dot_general(
            cin[part], bin_ref[part, :], (((1,), (1,)), ((), ())), preferred_element_type=F32
        )
        rows = cum_ref[0, 8 * block : 8 * block + 8, :]
        columns = jnp.transpose(rows)
        for head in range(RATIO):
            spread = columns[:, head : head + 1] - rows[head : head + 1, :]
            decay = jnp.exp(jnp.where(causal, spread, -jnp.inf))
            weights = (scores * decay * rows[RATIO + head : RATIO + head + 1, :]).astype(BF16)
            cols = slice(head * HEAD_DIM, (head + 1) * HEAD_DIM)
            inner_ref[part, cols] = jnp.dot(
                weights, xin_ref[part, cols], preferred_element_type=F32
            )


def scan_kernel(shared_ref, local_ref, out_ref):
    me = lax.axis_index("sp")
    pair = me // 2
    count = local_ref.shape[0]
    sums = jnp.concatenate(
        [
            jnp.sum(shared_ref[rank, 0:COMMON, :].astype(F32)[10:13], axis=0, keepdims=True)
            for rank in range(count)
        ],
        axis=0,
    )
    lane = lax.broadcasted_iota(jnp.int32, sums.shape, 1)
    for upper in range(2):
        ends = []
        for head in range(2):
            mine = jnp.sum(
                jnp.where(lane == count * upper + 2 * pair + head, sums, 0.0),
                axis=1,
                keepdims=True,
            )
            logs = shared_ref[8 * upper + pair, 0:COMMON, :].astype(F32)
            logs = logs[4 + 3 * head : 7 + 3 * head]
            rate = jnp.exp(logs[0:1] + logs[1:2] + logs[2:3])
            ends.append(jnp.exp(-rate * mine))
        decay = jnp.where(lane < HEAD_DIM, ends[0], ends[1])
        entering = jnp.zeros(local_ref.shape[1:], F32)
        for step in range(count // 2):
            slot = 2 * step + upper
            out_ref[slot] = entering.astype(BF16)
            if step + 1 < count // 2:
                passed = decay[2 * step : 2 * step + 1, :] * decay[2 * step + 1 : 2 * step + 2, :]
                entering = entering * passed + local_ref[slot].astype(F32)


def core_of(block, pair, ent_ref, first_ref, cin_ref, inner_ref, cum_ref):
    tokens = cin_ref.shape[0] // 2
    group, half = pair // 2, pair % 2
    rows = cum_ref[group]
    picked = jnp.where(block == 0, rows[0:8], rows[8:16])
    columns = jnp.transpose(jnp.exp(picked))
    cols = slice(half * STATE, (half + 1) * STATE)
    passed = head_row(jnp.exp(rows[0:RATIO, tokens - 1 : tokens]))[:, cols]
    entering = ent_ref[pair].astype(F32) * jnp.where(block == 0, 1.0, passed) + jnp.where(
        block == 0, 0.0, first_ref[pair]
    )
    part = pl.ds(pl.multiple_of(block * tokens, tokens), tokens)
    carried = jnp.dot(
        cin_ref[part, group * STATE : (group + 1) * STATE],
        entering.astype(BF16),
        preferred_element_type=F32,
    )
    inner = inner_ref[part, pair * STATE : (pair + 1) * STATE]
    return (inner + carried * per_head(columns, 2 * half)).astype(BF16)


def average_of():
    row_id = lax.broadcasted_iota(jnp.int32, (STATE, STATE), 0) // HEAD_DIM
    col_id = lax.broadcasted_iota(jnp.int32, (STATE, STATE), 1) // HEAD_DIM
    return jnp.where(row_id == col_id, 1.0 / HEAD_DIM, 0.0).astype(BF16)


def gate_norm(core, gate, gain, average):
    v = core.astype(F32) * silu(gate.astype(F32))
    squares = v * v
    high = squares.astype(BF16)
    low = (squares - high.astype(F32)).astype(BF16)
    mean = jnp.dot(high, average, preferred_element_type=F32) + jnp.dot(
        low, average, preferred_element_type=F32
    )
    return v * lax.rsqrt(mean + NORM_EPS) * gain


def give_kernel(ent_ref, first_ref, cin_ref, inner_ref, cum_ref, core_ref):
    block = 1 - lax.rem(lax.axis_index("sp"), 2)
    for pair in range(ent_ref.shape[0]):
        core_ref[:, pair * STATE : (pair + 1) * STATE] = core_of(
            block, pair, ent_ref, first_ref, cin_ref, inner_ref, cum_ref
        )


def mine_kernel(
    ent_ref, first_ref, cin_ref, inner_ref, cum_ref, z_ref, gain_ref, normed_ref
):
    side = lax.rem(lax.axis_index("sp"), 2)
    average = average_of()
    pairs = ent_ref.shape[0]
    for pair in range(pairs):
        core = core_of(side, pair, ent_ref, first_ref, cin_ref, inner_ref, cum_ref)
        cols = lanes((side * pairs + pair) * STATE, STATE)
        normed_ref[pair] = gate_norm(core, z_ref[:, cols], gain_ref[:, cols], average).astype(BF16)


def join_kernel(a_ref, b_ref, c_ref, d_ref, out_ref):
    rows = a_ref.shape[0]
    for k, ref in enumerate((a_ref, b_ref, c_ref, d_ref)):
        out_ref[k * rows : (k + 1) * rows, :] = ref[...]


def out_kernel(
    core_ref, near_ref, z_ref, gain_ref,
    m0_ref, m1_ref, m2_ref, m3_ref, o0_ref, o1_ref, o2_ref, o3_ref,
    out_ref, normed_ref, ordered_ref, held_ref, acc_ref, sems,
):
    rank = lax.axis_index("dp")
    y, x, core = rank // 8, lax.rem(rank // 2, 4), lax.rem(rank, 2)
    side = lax.rem(lax.axis_index("sp"), 2)
    pieces = (m0_ref, m1_ref, m2_ref, m3_ref, o0_ref, o1_ref, o2_ref, o3_ref)
    deep = m0_ref.shape[0]
    copies = [
        pltpu.make_async_copy(ref, held_ref.at[k * deep : (k + 1) * deep, :], sems.at[k])
        for k, ref in enumerate(pieces)
    ]
    for copy in copies:
        copy.start()
    average = average_of()
    pairs = near_ref.shape[0]
    for pair in range(pairs):
        normed_ref[side * pairs + pair] = near_ref[pair].astype(F32)
        far = (1 - side) * pairs + pair
        cols = lanes(far * STATE, STATE)
        value = gate_norm(
            core_ref[:, pair * STATE : (pair + 1) * STATE],
            z_ref[:, cols],
            gain_ref[:, cols],
            average,
        )
        normed_ref[far] = value
    tokens = out_ref.shape[0]
    lane = lax.broadcasted_iota(jnp.int32, (tokens, STATE), 1)

    def chip(side, position):
        major, minor = position // 4, position % 4
        ry = jnp.where(side == 0, major, minor)
        rx = jnp.where(side == 0, minor, major)
        return lax.rem(y + 4 - ry, 4) * 4 + lax.rem(x + 4 - rx, 4)

    for half, side in enumerate((core, 1 - core)):
        for k in range(8):
            left = normed_ref[chip(side, 2 * k)]
            right = normed_ref[chip(side, 2 * k + 1)]
            turned = pltpu.roll(jnp.where(side == 0, right, left), HEAD_DIM, 1)
            left = jnp.where(side == 0, left, turned)
            right = jnp.where(side == 0, turned, right)
            first = (half * 8 + k) * STATE
            ordered_ref[:, first : first + STATE] = jnp.where(
                lane < HEAD_DIM, left, right
            ).astype(BF16)
    chunk = 512
    stages = 4
    depth = held_ref.shape[0] // stages
    for stage in range(stages):
        for copy in copies[stage * 8 // stages : (stage + 1) * 8 // stages]:
            copy.wait()
        rows = slice(stage * depth, (stage + 1) * depth)
        for first in range(0, out_ref.shape[1], chunk):
            cols = slice(first, first + chunk)
            part = jnp.dot(
                ordered_ref[:, rows], held_ref[rows, cols], preferred_element_type=F32
            )
            if stage:
                part = part + acc_ref[:, cols]
            if stage < stages - 1:
                acc_ref[:, cols] = part
            else:
                out_ref[:, cols] = part.astype(BF16)


def vmem():
    return pl.BlockSpec(memory_space=pltpu.VMEM)


def in_hbm(*values):
    return [pltpu.with_memory_space_constraint(v, pltpu.HBM) for v in values]


def cost(flops, moved, special):
    return pl.CostEstimate(flops=flops, bytes_accessed=moved, transcendentals=special)


def first_step(y, x, core, d):
    return (y, x + d, core) if core == 0 else (y + d, x, core)


def second_step(y, x, core, d):
    return (y + d, x, core) if core == 0 else (y, x + d, core)


def swap_step(y, x, core, d):
    return y, x, 1 - core


def torus(step, d):
    pairs = []
    for rank in range(32):
        y, x, core = step(rank // 8, rank // 2 % 4, rank % 2, d)
        pairs.append((rank, ((y % 4) * 4 + x % 4) * 2 + core))
    return pairs


def step(
    stream_x, stream_b, stream_c, gate_z, step_raw,
    conv_x, conv_b, conv_c, decay_log, norm_gain, w_out,
):
    ranks = lax.axis_size("sp")
    x, b, c, z, raw = (v[0] for v in (stream_x, stream_b, stream_c, gate_z, step_raw))
    tokens, inner_width = x.shape
    wide, thin = inner_width // 2, b.shape[1] // 2
    groups = thin // STATE
    pairs = wide // STATE
    swap = [(i, i ^ 1) for i in range(ranks)]
    x, b, c, raw, taps = in_hbm(x, b, c, jnp.transpose(raw), conv_x)

    cols = wide + thin
    small, dt, own, give, own_c, give_c = pl.pallas_call(
        share_kernel,
        in_specs=[pl.BlockSpec(memory_space=pltpu.SMEM)] + [vmem()] * 5,
        out_specs=[vmem()] * 6,
        out_shape=[
            jax.ShapeDtypeStruct((ranks, COMMON + REACH * (cols + thin) // STATE, STATE), BF16),
            jax.ShapeDtypeStruct((2 * groups, 2 * RATIO, tokens), F32),
            jax.ShapeDtypeStruct((tokens, cols), BF16),
            jax.ShapeDtypeStruct((tokens + EXTRA, cols), BF16),
            jax.ShapeDtypeStruct((tokens, thin), BF16),
            jax.ShapeDtypeStruct((tokens, thin), BF16),
        ],
        compiler_params=pltpu.CompilerParams(vmem_limit_bytes=8 * MIB),
        cost_estimate=cost(10_000_000, 2_000_000, 10_000),
        name="share",
    )(decay_log, raw, taps, x, b, c)
    shared = lax.all_to_all(small, "sp", 0, 0, tiled=True)
    got = lax.ppermute(give, "sp", swap)
    got_c = lax.ppermute(give_c, "sp", swap)

    w1, w2, w3 = (lax.ppermute(w_out, "dp", torus(first_step, d)) for d in (1, 2, 3))
    row = pl.pallas_call(
        join_kernel,
        in_specs=[vmem()] * 4,
        out_specs=vmem(),
        out_shape=jax.ShapeDtypeStruct((4 * w_out.shape[0], w_out.shape[1]), BF16),
        compiler_params=pltpu.CompilerParams(vmem_limit_bytes=8 * MIB),
        cost_estimate=cost(1_000_000, 2_000_000, 0),
        name="join",
    )(w_out, w1, w2, w3)
    mine = [row] + [lax.ppermute(row, "dp", torus(second_step, d)) for d in (1, 2, 3)]
    other = [lax.ppermute(v, "dp", torus(swap_step, 0)) for v in mine]

    steps = pl.pallas_call(
        early_kernel,
        grid=(1,),
        in_specs=[
            pl.BlockSpec((EXTRA, cols), lambda i: (tokens // EXTRA, 0)),
            pl.BlockSpec(dt.shape, lambda i: (0, 0, 0)),
        ],
        out_specs=pl.BlockSpec((groups, 4 * RATIO, tokens), lambda i: (0, 0, 0)),
        out_shape=jax.ShapeDtypeStruct((groups, 4 * RATIO, tokens), F32),
        compiler_params=pltpu.CompilerParams(vmem_limit_bytes=8 * MIB),
        cost_estimate=cost(100_000_000, 100_000, 20_000),
        name="early",
    )(got, dt)

    per = 2
    away = wide // (per * STATE)
    state, first, xin, bin_, cum = pl.pallas_call(
        state_kernel,
        grid=(groups // per,),
        in_specs=[
            pl.BlockSpec((tokens, per * WIDTH), lambda g: (0, g)),
            pl.BlockSpec((tokens, per * STATE), lambda g: (0, away + g)),
            pl.BlockSpec((tokens + EXTRA, per * WIDTH), lambda g: (0, g)),
            pl.BlockSpec((tokens + EXTRA, per * STATE), lambda g: (0, away + g)),
            pl.BlockSpec(shared.shape, lambda g: (0, 0, 0)),
            pl.BlockSpec((4, 2 * thin), lambda g: (0, 0)),
            pl.BlockSpec((per, 4 * RATIO, tokens), lambda g: (g, 0, 0)),
        ],
        out_specs=[
            pl.BlockSpec((4 * per, HEAD_DIM, STATE), lambda g: (g, 0, 0)),
            pl.BlockSpec((2 * per, STATE, STATE), lambda g: (g, 0, 0)),
            pl.BlockSpec((2 * tokens, per * WIDTH), lambda g: (0, g)),
            pl.BlockSpec((2 * tokens, per * STATE), lambda g: (0, g)),
            pl.BlockSpec((per, 4 * RATIO, tokens), lambda g: (g, 0, 0)),
        ],
        out_shape=[
            jax.ShapeDtypeStruct((ranks, HEAD_DIM, STATE), BF16),
            pltpu.HBM((pairs, STATE, STATE), F32),
            pltpu.HBM((2 * tokens, wide), BF16),
            pltpu.HBM((2 * tokens, thin), BF16),
            pltpu.HBM((groups, 4 * RATIO, tokens), F32),
        ],
        scratch_shapes=[
            pltpu.VMEM((per, PAD + 2 * tokens, WIDTH), F32),
            pltpu.VMEM((per, PAD + 2 * tokens, STATE), F32),
        ],
        compiler_params=pltpu.CompilerParams(vmem_limit_bytes=16 * MIB),
        cost_estimate=cost(4_000_000_000, 2_000_000, 400_000),
        name="state",
    )(own, own, got, got, shared, conv_b, steps)

    local = lax.all_to_all(state, "sp", 0, 0, tiled=True)

    cin, inner = pl.pallas_call(
        inner_kernel,
        grid=(groups,),
        in_specs=[
            pl.BlockSpec((tokens, STATE), lambda g: (0, g)),
            pl.BlockSpec((tokens, STATE), lambda g: (0, g)),
            pl.BlockSpec(shared.shape, lambda g: (0, 0, 0)),
            pl.BlockSpec((4, 2 * thin), lambda g: (0, 0)),
            pl.BlockSpec((2 * tokens, STATE), lambda g: (0, g)),
            pl.BlockSpec((2 * tokens, WIDTH), lambda g: (0, g)),
            pl.BlockSpec((1, 4 * RATIO, tokens), lambda g: (g, 0, 0)),
        ],
        out_specs=[
            pl.BlockSpec((2 * tokens, STATE), lambda g: (0, g)),
            pl.BlockSpec((2 * tokens, WIDTH), lambda g: (0, g)),
        ],
        out_shape=[
            pltpu.HBM((2 * tokens, thin), BF16),
            pltpu.HBM((2 * tokens, wide), F32),
        ],
        scratch_shapes=[pltpu.VMEM((PAD + 2 * tokens, STATE), F32)],
        compiler_params=pltpu.CompilerParams(vmem_limit_bytes=16 * MIB),
        cost_estimate=cost(4_000_000_000, 2_000_000, 700_000),
        name="inner",
    )(own_c, got_c, shared, conv_c, *in_hbm(bin_, xin, cum))

    entering = pl.pallas_call(
        scan_kernel,
        in_specs=[vmem(), vmem()],
        out_specs=vmem(),
        out_shape=jax.ShapeDtypeStruct(local.shape, BF16),
        compiler_params=pltpu.CompilerParams(vmem_limit_bytes=8 * MIB),
        cost_estimate=cost(1_000_000_000, 1_000_000, 0),
        name="scan",
    )(shared, local)
    entering = lax.all_to_all(entering, "sp", 0, 0, tiled=True)
    entering = entering.reshape(pairs, STATE, STATE)

    mixer = (entering, *in_hbm(first, cin, inner, cum))
    core = pl.pallas_call(
        give_kernel,
        in_specs=[vmem()] * 5,
        out_specs=vmem(),
        out_shape=jax.ShapeDtypeStruct((tokens, wide), BF16),
        compiler_params=pltpu.CompilerParams(vmem_limit_bytes=8 * MIB),
        cost_estimate=cost(1_000_000_000, 1_000_000, 0),
        name="give",
    )(*mixer)
    got_core = lax.ppermute(core, "sp", swap)
    gain = norm_gain[None]
    normed = pl.pallas_call(
        mine_kernel,
        in_specs=[vmem()] * 7,
        out_specs=vmem(),
        out_shape=jax.ShapeDtypeStruct((pairs, tokens, STATE), BF16),
        compiler_params=pltpu.CompilerParams(vmem_limit_bytes=8 * MIB),
        cost_estimate=cost(2_000_000_000, 1_000_000, 0),
        name="mine",
    )(*mixer, z, gain)
    mixed = pl.pallas_call(
        out_kernel,
        in_specs=[vmem()] * 4 + [pl.BlockSpec(memory_space=pltpu.HBM)] * 4 + [pl.BlockSpec(memory_space=pl.ANY)] * 4,
        out_specs=vmem(),
        out_shape=jax.ShapeDtypeStruct((tokens, w_out.shape[1]), BF16),
        scratch_shapes=[
            pltpu.VMEM((2 * pairs, tokens, STATE), F32),
            pltpu.VMEM((tokens, inner_width), BF16),
            pltpu.VMEM((inner_width, w_out.shape[1]), BF16),
            pltpu.VMEM((tokens, w_out.shape[1]), F32),
            pltpu.SemaphoreType.DMA((8,)),
        ],
        compiler_params=pltpu.CompilerParams(vmem_limit_bytes=OUT_LIMIT),
        cost_estimate=cost(4_000_000_000, 10_000_000, 300_000),
        name="project",
    )(got_core, normed, z, gain, *in_hbm(*mine), *other)
    return mixed[None]


def solution(mesh):
    placed = (
        P("dp", "sp", None),
        P("dp", "sp", None),
        P("dp", "sp", None),
        P("dp", "sp", None),
        P("dp", "sp", None),
        P(None, "sp"),
        P(),
        P(),
        P("sp"),
        P(),
        P("dp", None),
    )
    return jax.shard_map(
        step, mesh=mesh, in_specs=placed, out_specs=P("dp", "sp", None), check_vma=False
    )
```

```python
import jax
import jax.numpy as jnp
from jax import lax
from jax.experimental import pallas as pl
from jax.experimental.pallas import tpu as pltpu
from jax.sharding import PartitionSpec as P


HEAD_DIM = 64
STATE = 128
RATIO = 4
WIDTH = RATIO * HEAD_DIM
NORM_EPS = 1.0
HIGHEST = lax.Precision.HIGHEST
F32 = jnp.float32
BF16 = jnp.bfloat16
HALO = 4
EXTRA = 8
REACH = 3
COMMON = 16
PAD = 8
MIB = 1 << 20
OUT_LIMIT = 20 * MIB


def silu(u):
    half = 0.5 * u
    return half + half * jnp.tanh(half)


def lanes(first, size):
    return pl.ds(pl.multiple_of(first, STATE), size)


def conv_silu(pad_ref, halo, own, given, side, taps):
    tokens = own.shape[0]
    rows = 2 * tokens
    pad_ref[PAD - HALO : PAD, :] = halo.astype(F32)
    pad_ref[pl.ds(pl.multiple_of(PAD + side * tokens, 8), tokens), :] = own.astype(F32)
    pad_ref[pl.ds(pl.multiple_of(PAD + (1 - side) * tokens, 8), tokens), :] = given.astype(F32)
    total = taps[3:4, :] * pad_ref[PAD : PAD + rows, :]
    for back in range(1, 4):
        total = total + taps[3 - back : 4 - back, :] * pad_ref[PAD - back : PAD - back + rows, :]
    return silu(total)


def per_head(columns, first):
    tokens = columns.shape[0]
    lane = lax.broadcasted_iota(jnp.int32, (tokens, 128), 1)
    left = jnp.broadcast_to(columns[:, first : first + 1], (tokens, 128))
    right = jnp.broadcast_to(columns[:, first + 1 : first + 2], (tokens, 128))
    return jnp.where(lane < HEAD_DIM, left, right)


def head_row(values):
    lane = lax.broadcasted_iota(jnp.int32, (1, WIDTH), 1)
    row = jnp.broadcast_to(values[0:1], (1, WIDTH))
    for head in range(1, RATIO):
        row = jnp.where(
            lane >= head * HEAD_DIM, jnp.broadcast_to(values[head : head + 1], (1, WIDTH)), row
        )
    return row


def steps_of(raw):
    tokens = raw.shape[1]
    raw = raw.astype(F32)
    dt = jnp.maximum(raw, 0.0) + jnp.log1p(jnp.exp(-jnp.abs(raw)))
    src = lax.broadcasted_iota(jnp.int32, (tokens, tokens), 0)
    dst = lax.broadcasted_iota(jnp.int32, (tokens, tokens), 1)
    upper = (src <= dst).astype(F32)
    return dt, jnp.dot(dt, upper, precision=HIGHEST, preferred_element_type=F32)


def thirds(value):
    high = value.astype(BF16).astype(F32)
    rest = value - high
    middle = rest.astype(BF16).astype(F32)
    return [high, middle, rest - middle]


def share_kernel(
    logs_ref, raw_ref, taps_ref, x_ref, b_ref, c_ref,
    small_ref, dt_ref, own_ref, give_ref, own_c_ref, give_c_ref,
):
    heads, tokens = raw_ref.shape
    side = lax.rem(lax.axis_index("sp"), 2)
    other = 1 - side
    raw = raw_ref[...].astype(F32)
    left = 0
    for source in (x_ref, b_ref):
        half = source.shape[1] // 2
        own_ref[:, left : left + half] = source[:, lanes(side * half, half)]
        give_ref[0:tokens, left : left + half] = source[:, lanes(other * half, half)]
        left += half
    half = c_ref.shape[1] // 2
    own_c_ref[...] = c_ref[:, lanes(side * half, half)]
    give_c_ref[...] = c_ref[:, lanes(other * half, half)]
    theirs = jnp.where(other == 0, raw[0 : heads // 2], raw[heads // 2 :])
    per = left // tokens
    flats = []
    for first in range(0, heads // 2, per):
        held = min(per, heads // 2 - first)
        flats.append(
            jnp.concatenate(
                [theirs[first + k : first + k + 1] for k in range(held)]
                + [jnp.zeros((1, tokens), F32)] * (per - held),
                axis=1,
            )
        )
    flats.append(jnp.zeros((EXTRA - len(flats), left), F32))
    give_ref[tokens : tokens + EXTRA, :] = jnp.concatenate(flats, axis=0).astype(BF16)

    dt, prefix = steps_of(raw)
    for group in range(heads // RATIO):
        rows = slice(group * RATIO, (group + 1) * RATIO)
        dt_ref[group, 0:RATIO, :] = prefix[rows]
        dt_ref[group, RATIO:, :] = dt[rows]
    ones = jnp.ones((8, tokens), F32)
    sums = lax.dot_general(
        ones, dt, (((1,), (1,)), ((), ())), precision=HIGHEST, preferred_element_type=F32
    )
    sums = jnp.concatenate([sums[0:1], jnp.zeros((1, 128 - heads), F32)], axis=1)
    common = jnp.concatenate(
        [taps_ref[...].astype(F32)]
        + thirds(jnp.broadcast_to(logs_ref[:, 0:1], (1, 128)))
        + thirds(jnp.broadcast_to(logs_ref[:, 1:2], (1, 128)))
        + thirds(sums)
        + [jnp.zeros((3, 128), F32)],
        axis=0,
    ).astype(BF16)
    ends = []
    for part in range(2):
        rows = []
        tails = [ref[tokens - 8 :, :].astype(F32) for ref in (x_ref, b_ref, c_ref)]
        for token in range(8 - REACH, 8):
            for tail in tails:
                half = tail.shape[1] // 2
                for first in range(part * half, (part + 1) * half, STATE):
                    rows.append(tail[token : token + 1, first : first + STATE])
        ends.append(jnp.concatenate(rows, axis=0).astype(BF16))
    for rank in range(small_ref.shape[0]):
        small_ref[rank, 0:COMMON, :] = common
        small_ref[rank, COMMON:, :] = ends[rank % 2]


def halo_of(shared_ref, first, count):
    pair = lax.axis_index("sp") // 2
    source = jnp.maximum(2 * pair - 1, 0)
    ends = shared_ref[source, COMMON:, :].astype(F32)
    ends = jnp.where(pair == 0, 0.0, ends)
    stride = ends.shape[0] // REACH
    row_id = lax.broadcasted_iota(jnp.int32, ends.shape, 0)
    rows = [jnp.zeros((HALO - REACH, count * STATE), F32)]
    for token in range(REACH):
        picked = [
            jnp.sum(
                jnp.where(row_id == token * stride + first + k, ends, 0.0), axis=0, keepdims=True
            )
            for k in range(count)
        ]
        rows.append(jnp.concatenate(picked, axis=1))
    return jnp.concatenate(rows, axis=0)


def early_kernel(got_ref, dt_ref, steps_ref):
    side = lax.rem(lax.axis_index("sp"), 2)
    groups, _, tokens = steps_ref.shape
    flat = got_ref[...].astype(F32)
    per = flat.shape[1] // tokens
    raw = jnp.concatenate(
        [
            flat[k // per : k // per + 1, k % per * tokens : (k % per + 1) * tokens]
            for k in range(groups * RATIO)
        ],
        axis=0,
    )
    dt, prefix = steps_of(raw)
    for group in range(groups):
        rows = slice(group * RATIO, (group + 1) * RATIO)
        given = jnp.concatenate([prefix[rows], dt[rows]], axis=0)
        own = dt_ref[side * groups + group]
        steps_ref[group, 0 : 2 * RATIO, :] = jnp.where(side == 0, own, given)
        steps_ref[group, 2 * RATIO :, :] = jnp.where(side == 0, given, own)


def state_kernel(
    own_ref, own_b_ref, got_ref, got_b_ref, shared_ref, tb_ref, steps_ref,
    state_ref, first_ref, xin_ref, bin_ref, cum_ref, pad_ref, pad_b_ref,
):
    side = lax.rem(lax.axis_index("sp"), 2)
    tokens = own_ref.shape[0]
    end = tokens - 1
    per = steps_ref.shape[0]
    for k in range(per):
        wide = slice(k * WIDTH, (k + 1) * WIDTH)
        thin = slice(k * STATE, (k + 1) * STATE)
        group = per * pl.program_id(0) + k
        piece = 8 * side + 2 * group
        lower = shared_ref[piece, 0:COMMON, :].astype(F32)
        upper = shared_ref[piece + 1, 0:COMMON, :].astype(F32)
        rows = steps_ref[k]
        logs = []
        for part in (lower, upper):
            for row in (4, 7):
                logs.append(part[row : row + 1] + part[row + 1 : row + 2] + part[row + 2 : row + 3])
        rate = jnp.exp(jnp.concatenate(logs, axis=0))
        cums, tails = [], []
        for block in range(2):
            prefix = rows[8 * block : 8 * block + RATIO]
            dt = rows[8 * block + RATIO : 8 * block + 2 * RATIO]
            cum = -rate * prefix
            cums += [cum, dt]
            tails.append(jnp.exp(cum[:, end : end + 1] - cum) * dt)
        cum_ref[k] = jnp.concatenate(cums, axis=0)
        columns = jnp.transpose(jnp.concatenate(tails, axis=0))
        xin = conv_silu(
            pad_ref.at[k],
            halo_of(shared_ref, 2 * group, 2),
            own_ref[:, wide],
            got_ref[0:tokens, wide],
            side,
            jnp.concatenate([lower[0:4], upper[0:4]], axis=1),
        ).astype(BF16)
        bin_ = conv_silu(
            pad_b_ref.at[k],
            halo_of(shared_ref, 8 + group, 1),
            own_b_ref[:, thin],
            got_b_ref[0:tokens, thin],
            side,
            tb_ref[:, lanes((side * 4 + group) * STATE, STATE)].astype(F32),
        ).astype(BF16)
        bin_ref[:, thin] = bin_
        xin_ref[:, wide] = xin
        states = []
        for block in range(2):
            part = slice(block * tokens, (block + 1) * tokens)
            scale = jnp.concatenate(
                [per_head(columns, 4 * block), per_head(columns, 4 * block + 2)], axis=1
            )
            scaled = (xin[part].astype(F32) * scale).astype(BF16)
            states.append(
                lax.dot_general(
                    bin_[part],
                    scaled,
                    (((0,), (0,)), ((), ())),
                    preferred_element_type=F32,
                )
            )
        both = (states[1] + states[0] * head_row(jnp.exp(cums[2][:, end : end + 1]))).astype(BF16)
        for half in range(2):
            cols = slice(half * STATE, (half + 1) * STATE)
            first_ref[2 * k + half] = states[0][:, cols].astype(BF16)
            for part in range(2):
                state_ref[4 * k + 2 * half + part] = both[
                    part * HEAD_DIM : (part + 1) * HEAD_DIM, cols
                ]


def inner_kernel(
    own_ref, got_ref, shared_ref, tc_ref, bin_ref, xin_ref, cum_ref,
    cin_ref, inner_ref, pad_ref,
):
    side = lax.rem(lax.axis_index("sp"), 2)
    group = pl.program_id(0)
    groups = pl.num_programs(0)
    tokens = own_ref.shape[0]
    cin = conv_silu(
        pad_ref,
        halo_of(shared_ref, 12 + group, 1),
        own_ref[...],
        got_ref[...],
        side,
        tc_ref[:, lanes((side * groups + group) * STATE, STATE)].astype(F32),
    ).astype(BF16)
    cin_ref[...] = cin
    row_id = lax.broadcasted_iota(jnp.int32, (tokens, tokens), 0)
    col_id = lax.broadcasted_iota(jnp.int32, (tokens, tokens), 1)
    causal = row_id >= col_id
    for block in range(2):
        part = slice(block * tokens, (block + 1) * tokens)
        scores = lax.dot_general(
            cin[part], bin_ref[part, :], (((1,), (1,)), ((), ())), preferred_element_type=F32
        )
        rows = cum_ref[0, 8 * block : 8 * block + 8, :]
        columns = jnp.transpose(rows)
        for head in range(RATIO):
            spread = columns[:, head : head + 1] - rows[head : head + 1, :]
            decay = jnp.exp(jnp.where(causal, spread, -jnp.inf))
            weights = (scores * decay * rows[RATIO + head : RATIO + head + 1, :]).astype(BF16)
            cols = slice(head * HEAD_DIM, (head + 1) * HEAD_DIM)
            inner_ref[part, cols] = jnp.dot(
                weights, xin_ref[part, cols], preferred_element_type=F32
            )


def scan_kernel(shared_ref, local_ref, out_ref):
    me = lax.axis_index("sp")
    pair = me // 2
    count = local_ref.shape[0]
    sums = jnp.concatenate(
        [
            jnp.sum(shared_ref[rank, 0:COMMON, :].astype(F32)[10:13], axis=0, keepdims=True)
            for rank in range(count)
        ],
        axis=0,
    )
    lane = lax.broadcasted_iota(jnp.int32, sums.shape, 1)
    for upper in range(2):
        ends = []
        for head in range(2):
            mine = jnp.sum(
                jnp.where(lane == count * upper + 2 * pair + head, sums, 0.0),
                axis=1,
                keepdims=True,
            )
            logs = shared_ref[8 * upper + pair, 0:COMMON, :].astype(F32)
            logs = logs[4 + 3 * head : 7 + 3 * head]
            rate = jnp.exp(logs[0:1] + logs[1:2] + logs[2:3])
            ends.append(jnp.exp(-rate * mine))
        decay = jnp.where(lane < HEAD_DIM, ends[0], ends[1])
        entering = jnp.zeros(local_ref.shape[1:], F32)
        for step in range(count // 2):
            slot = 2 * step + upper
            out_ref[slot] = entering.astype(BF16)
            if step + 1 < count // 2:
                passed = decay[2 * step : 2 * step + 1, :] * decay[2 * step + 1 : 2 * step + 2, :]
                entering = entering * passed + local_ref[slot].astype(F32)


def core_of(block, pair, ent_ref, first_ref, cin_ref, inner_ref, cum_ref):
    tokens = cin_ref.shape[0]
    group, half = pair // 2, pair % 2
    rows = cum_ref[group]
    picked = jnp.where(block == 0, rows[0:8], rows[8:16])
    columns = jnp.transpose(jnp.exp(picked))
    cols = slice(half * STATE, (half + 1) * STATE)
    passed = head_row(jnp.exp(rows[0:RATIO, tokens - 1 : tokens]))[:, cols]
    entering = ent_ref[pair].astype(F32) * jnp.where(block == 0, 1.0, passed) + jnp.where(
        block == 0, 0.0, first_ref[pair].astype(F32)
    )
    carried = jnp.dot(
        cin_ref[:, group * STATE : (group + 1) * STATE],
        entering.astype(BF16),
        preferred_element_type=F32,
    )
    inner = inner_ref[:, pair * STATE : (pair + 1) * STATE]
    return (inner + carried * per_head(columns, 2 * half)).astype(BF16)


def average_of():
    row_id = lax.broadcasted_iota(jnp.int32, (STATE, STATE), 0) // HEAD_DIM
    col_id = lax.broadcasted_iota(jnp.int32, (STATE, STATE), 1) // HEAD_DIM
    return jnp.where(row_id == col_id, 1.0 / HEAD_DIM, 0.0).astype(BF16)


def gate_norm(core, gate, gain, average):
    v = core.astype(F32) * silu(gate.astype(F32))
    squares = v * v
    high = squares.astype(BF16)
    low = (squares - high.astype(F32)).astype(BF16)
    mean = jnp.dot(high, average, preferred_element_type=F32) + jnp.dot(
        low, average, preferred_element_type=F32
    )
    return v * lax.rsqrt(mean + NORM_EPS) * gain


def give_kernel(ent_ref, first_ref, cin_ref, inner_ref, cum_ref, core_ref):
    block = 1 - lax.rem(lax.axis_index("sp"), 2)
    for pair in range(ent_ref.shape[0]):
        core_ref[:, pair * STATE : (pair + 1) * STATE] = core_of(
            block, pair, ent_ref, first_ref, cin_ref, inner_ref, cum_ref
        )


def mine_kernel(
    ent_ref, first_ref, cin_ref, inner_ref, cum_ref, z_ref, gain_ref, normed_ref
):
    side = lax.rem(lax.axis_index("sp"), 2)
    average = average_of()
    pairs = ent_ref.shape[0]
    for pair in range(pairs):
        core = core_of(side, pair, ent_ref, first_ref, cin_ref, inner_ref, cum_ref)
        cols = lanes((side * pairs + pair) * STATE, STATE)
        normed_ref[pair] = gate_norm(core, z_ref[:, cols], gain_ref[:, cols], average).astype(BF16)


def join_kernel(a_ref, b_ref, c_ref, d_ref, out_ref):
    rows = a_ref.shape[0]
    for k, ref in enumerate((a_ref, b_ref, c_ref, d_ref)):
        out_ref[k * rows : (k + 1) * rows, :] = ref[...]


def out_kernel(
    core_ref, near_ref, z_ref, gain_ref,
    m0_ref, m1_ref, m2_ref, m3_ref, o0_ref, o1_ref, o2_ref, o3_ref,
    out_ref, normed_ref, ordered_ref, held_ref, acc_ref, sems,
):
    rank = lax.axis_index("dp")
    y, x, core = rank // 8, lax.rem(rank // 2, 4), lax.rem(rank, 2)
    side = lax.rem(lax.axis_index("sp"), 2)
    pieces = (m0_ref, m1_ref, m2_ref, m3_ref, o0_ref, o1_ref, o2_ref, o3_ref)
    deep = m0_ref.shape[0]
    copies = [
        pltpu.make_async_copy(ref, held_ref.at[k * deep : (k + 1) * deep, :], sems.at[k])
        for k, ref in enumerate(pieces)
    ]
    for copy in copies:
        copy.start()
    average = average_of()
    pairs = near_ref.shape[0]
    for pair in range(pairs):
        normed_ref[side * pairs + pair] = near_ref[pair].astype(F32)
        far = (1 - side) * pairs + pair
        cols = lanes(far * STATE, STATE)
        value = gate_norm(
            core_ref[:, pair * STATE : (pair + 1) * STATE],
            z_ref[:, cols],
            gain_ref[:, cols],
            average,
        )
        normed_ref[far] = value
    tokens = out_ref.shape[0]
    lane = lax.broadcasted_iota(jnp.int32, (tokens, STATE), 1)

    def chip(side, position):
        major, minor = position // 4, position % 4
        ry = jnp.where(side == 0, major, minor)
        rx = jnp.where(side == 0, minor, major)
        return lax.rem(y + 4 - ry, 4) * 4 + lax.rem(x + 4 - rx, 4)

    for half, side in enumerate((core, 1 - core)):
        for k in range(8):
            left = normed_ref[chip(side, 2 * k)]
            right = normed_ref[chip(side, 2 * k + 1)]
            turned = pltpu.roll(jnp.where(side == 0, right, left), HEAD_DIM, 1)
            left = jnp.where(side == 0, left, turned)
            right = jnp.where(side == 0, turned, right)
            first = (half * 8 + k) * STATE
            ordered_ref[:, first : first + STATE] = jnp.where(
                lane < HEAD_DIM, left, right
            ).astype(BF16)
    chunk = 512
    stages = 4
    depth = held_ref.shape[0] // stages
    for stage in range(stages):
        for copy in copies[stage * 8 // stages : (stage + 1) * 8 // stages]:
            copy.wait()
        rows = slice(stage * depth, (stage + 1) * depth)
        for first in range(0, out_ref.shape[1], chunk):
            cols = slice(first, first + chunk)
            part = jnp.dot(
                ordered_ref[:, rows], held_ref[rows, cols], preferred_element_type=F32
            )
            if stage:
                part = part + acc_ref[:, cols]
            if stage < stages - 1:
                acc_ref[:, cols] = part
            else:
                out_ref[:, cols] = part.astype(BF16)


def vmem():
    return pl.BlockSpec(memory_space=pltpu.VMEM)


def in_hbm(*values):
    return [pltpu.with_memory_space_constraint(v, pltpu.HBM) for v in values]


def cost(flops, moved, special):
    return pl.CostEstimate(flops=flops, bytes_accessed=moved, transcendentals=special)


def first_step(y, x, core, d):
    return (y, x + d, core) if core == 0 else (y + d, x, core)


def second_step(y, x, core, d):
    return (y + d, x, core) if core == 0 else (y, x + d, core)


def swap_step(y, x, core, d):
    return y, x, 1 - core


def torus(step, d):
    pairs = []
    for rank in range(32):
        y, x, core = step(rank // 8, rank // 2 % 4, rank % 2, d)
        pairs.append((rank, ((y % 4) * 4 + x % 4) * 2 + core))
    return pairs


def step(
    stream_x, stream_b, stream_c, gate_z, step_raw,
    conv_x, conv_b, conv_c, decay_log, norm_gain, w_out,
):
    ranks = lax.axis_size("sp")
    x, b, c, z, raw = (v[0] for v in (stream_x, stream_b, stream_c, gate_z, step_raw))
    tokens, inner_width = x.shape
    wide, thin = inner_width // 2, b.shape[1] // 2
    groups = thin // STATE
    pairs = wide // STATE
    swap = [(i, i ^ 1) for i in range(ranks)]
    x, b, c, raw, taps, logs = in_hbm(
        x, b, c, jnp.transpose(raw), conv_x, decay_log[None]
    )

    cols = wide + thin
    small, dt, own, give, own_c, give_c = pl.pallas_call(
        share_kernel,
        in_specs=[vmem()] * 6,
        out_specs=[vmem()] * 6,
        out_shape=[
            jax.ShapeDtypeStruct((ranks, COMMON + REACH * (cols + thin) // STATE, STATE), BF16),
            jax.ShapeDtypeStruct((2 * groups, 2 * RATIO, tokens), F32),
            jax.ShapeDtypeStruct((tokens, cols), BF16),
            jax.ShapeDtypeStruct((tokens + EXTRA, cols), BF16),
            jax.ShapeDtypeStruct((tokens, thin), BF16),
            jax.ShapeDtypeStruct((tokens, thin), BF16),
        ],
        compiler_params=pltpu.CompilerParams(vmem_limit_bytes=8 * MIB),
        cost_estimate=cost(10_000_000, 2_000_000, 10_000),
        name="share",
    )(logs, raw, taps, x, b, c)
    shared = lax.all_to_all(small, "sp", 0, 0, tiled=True)
    got = lax.ppermute(give, "sp", swap)
    got_c = lax.ppermute(give_c, "sp", swap)

    w1, w2, w3 = (lax.ppermute(w_out, "dp", torus(first_step, d)) for d in (1, 2, 3))
    row = pl.pallas_call(
        join_kernel,
        in_specs=[vmem()] * 4,
        out_specs=vmem(),
        out_shape=jax.ShapeDtypeStruct((4 * w_out.shape[0], w_out.shape[1]), BF16),
        compiler_params=pltpu.CompilerParams(vmem_limit_bytes=8 * MIB),
        cost_estimate=cost(1_000_000, 2_000_000, 0),
        name="join",
    )(w_out, w1, w2, w3)
    mine = [row] + [lax.ppermute(row, "dp", torus(second_step, d)) for d in (1, 2, 3)]
    other = [lax.ppermute(v, "dp", torus(swap_step, 0)) for v in mine]

    steps = pl.pallas_call(
        early_kernel,
        grid=(1,),
        in_specs=[
            pl.BlockSpec((EXTRA, cols), lambda i: (tokens // EXTRA, 0)),
            pl.BlockSpec(dt.shape, lambda i: (0, 0, 0)),
        ],
        out_specs=pl.BlockSpec((groups, 4 * RATIO, tokens), lambda i: (0, 0, 0)),
        out_shape=jax.ShapeDtypeStruct((groups, 4 * RATIO, tokens), F32),
        compiler_params=pltpu.CompilerParams(vmem_limit_bytes=8 * MIB),
        cost_estimate=cost(100_000_000, 100_000, 20_000),
        name="early",
    )(got, dt)

    per = 2
    away = wide // (per * STATE)
    state, first, xin, bin_, cum = pl.pallas_call(
        state_kernel,
        grid=(groups // per,),
        in_specs=[
            pl.BlockSpec((tokens, per * WIDTH), lambda g: (0, g)),
            pl.BlockSpec((tokens, per * STATE), lambda g: (0, away + g)),
            pl.BlockSpec((tokens + EXTRA, per * WIDTH), lambda g: (0, g)),
            pl.BlockSpec((tokens + EXTRA, per * STATE), lambda g: (0, away + g)),
            pl.BlockSpec(shared.shape, lambda g: (0, 0, 0)),
            pl.BlockSpec((4, 2 * thin), lambda g: (0, 0)),
            pl.BlockSpec((per, 4 * RATIO, tokens), lambda g: (g, 0, 0)),
        ],
        out_specs=[
            pl.BlockSpec((4 * per, HEAD_DIM, STATE), lambda g: (g, 0, 0)),
            pl.BlockSpec((2 * per, STATE, STATE), lambda g: (g, 0, 0)),
            pl.BlockSpec((2 * tokens, per * WIDTH), lambda g: (0, g)),
            pl.BlockSpec((2 * tokens, per * STATE), lambda g: (0, g)),
            pl.BlockSpec((per, 4 * RATIO, tokens), lambda g: (g, 0, 0)),
        ],
        out_shape=[
            jax.ShapeDtypeStruct((ranks, HEAD_DIM, STATE), BF16),
            pltpu.HBM((pairs, STATE, STATE), BF16),
            pltpu.HBM((2 * tokens, wide), BF16),
            pltpu.HBM((2 * tokens, thin), BF16),
            pltpu.HBM((groups, 4 * RATIO, tokens), F32),
        ],
        scratch_shapes=[
            pltpu.VMEM((per, PAD + 2 * tokens, WIDTH), F32),
            pltpu.VMEM((per, PAD + 2 * tokens, STATE), F32),
        ],
        compiler_params=pltpu.CompilerParams(vmem_limit_bytes=16 * MIB),
        cost_estimate=cost(4_000_000_000, 2_000_000, 400_000),
        name="state",
    )(own, own, got, got, shared, conv_b, steps)

    local = lax.all_to_all(state, "sp", 0, 0, tiled=True)

    cin, inner = pl.pallas_call(
        inner_kernel,
        grid=(groups,),
        in_specs=[
            pl.BlockSpec((tokens, STATE), lambda g: (0, g)),
            pl.BlockSpec((tokens, STATE), lambda g: (0, g)),
            pl.BlockSpec(shared.shape, lambda g: (0, 0, 0)),
            pl.BlockSpec((4, 2 * thin), lambda g: (0, 0)),
            pl.BlockSpec((2 * tokens, STATE), lambda g: (0, g)),
            pl.BlockSpec((2 * tokens, WIDTH), lambda g: (0, g)),
            pl.BlockSpec((1, 4 * RATIO, tokens), lambda g: (g, 0, 0)),
        ],
        out_specs=[
            pl.BlockSpec((2 * tokens, STATE), lambda g: (0, g)),
            pl.BlockSpec((2 * tokens, WIDTH), lambda g: (0, g)),
        ],
        out_shape=[
            pltpu.HBM((2 * tokens, thin), BF16),
            pltpu.HBM((2 * tokens, wide), F32),
        ],
        scratch_shapes=[pltpu.VMEM((PAD + 2 * tokens, STATE), F32)],
        compiler_params=pltpu.CompilerParams(vmem_limit_bytes=16 * MIB),
        cost_estimate=cost(4_000_000_000, 2_000_000, 700_000),
        name="inner",
    )(own_c, got_c, shared, conv_c, *in_hbm(bin_, xin, cum))

    entering = pl.pallas_call(
        scan_kernel,
        in_specs=[vmem(), vmem()],
        out_specs=vmem(),
        out_shape=jax.ShapeDtypeStruct(local.shape, BF16),
        compiler_params=pltpu.CompilerParams(vmem_limit_bytes=8 * MIB),
        cost_estimate=cost(1_000_000_000, 1_000_000, 0),
        name="scan",
    )(shared, local)
    entering = lax.all_to_all(entering, "sp", 0, 0, tiled=True)
    entering = entering.reshape(pairs, STATE, STATE)

    mixer = (entering, *in_hbm(first, cin, inner, cum))

    def whole(value):
        return pl.BlockSpec(value.shape, lambda i: (0,) * value.ndim)

    def half_of(value, theirs):
        def index(i):
            side = lax.rem(lax.axis_index("sp"), 2)
            return (1 - side if theirs else side, 0)

        return pl.BlockSpec((value.shape[0] // 2, value.shape[1]), index)

    def mixer_specs(theirs):
        return [
            whole(entering),
            whole(first),
            half_of(cin, theirs),
            half_of(inner, theirs),
            whole(cum),
        ]

    core = pl.pallas_call(
        give_kernel,
        grid=(1,),
        in_specs=mixer_specs(True),
        out_specs=pl.BlockSpec((tokens, wide), lambda i: (0, 0)),
        out_shape=jax.ShapeDtypeStruct((tokens, wide), BF16),
        compiler_params=pltpu.CompilerParams(vmem_limit_bytes=8 * MIB),
        cost_estimate=cost(1_000_000_000, 1_000_000, 0),
        name="give",
    )(*mixer)
    got_core = lax.ppermute(core, "sp", swap)
    gain = norm_gain[None]
    normed = pl.pallas_call(
        mine_kernel,
        grid=(1,),
        in_specs=mixer_specs(False) + [whole(z), whole(gain)],
        out_specs=pl.BlockSpec((pairs, tokens, STATE), lambda i: (0, 0, 0)),
        out_shape=jax.ShapeDtypeStruct((pairs, tokens, STATE), BF16),
        compiler_params=pltpu.CompilerParams(vmem_limit_bytes=8 * MIB),
        cost_estimate=cost(2_000_000_000, 1_000_000, 0),
        name="mine",
    )(*mixer, z, gain)
    mixed = pl.pallas_call(
        out_kernel,
        in_specs=[vmem()] * 4 + [pl.BlockSpec(memory_space=pltpu.HBM)] * 4 + [pl.BlockSpec(memory_space=pl.ANY)] * 4,
        out_specs=vmem(),
        out_shape=jax.ShapeDtypeStruct((tokens, w_out.shape[1]), BF16),
        scratch_shapes=[
            pltpu.VMEM((2 * pairs, tokens, STATE), F32),
            pltpu.VMEM((tokens, inner_width), BF16),
            pltpu.VMEM((inner_width, w_out.shape[1]), BF16),
            pltpu.VMEM((tokens, w_out.shape[1]), F32),
            pltpu.SemaphoreType.DMA((8,)),
        ],
        compiler_params=pltpu.CompilerParams(vmem_limit_bytes=OUT_LIMIT),
        cost_estimate=cost(4_000_000_000, 10_000_000, 300_000),
        name="project",
    )(got_core, normed, z, gain, *in_hbm(*mine), *other)
    return mixed[None]


def solution(mesh):
    placed = (
        P("dp", "sp", None),
        P("dp", "sp", None),
        P("dp", "sp", None),
        P("dp", "sp", None),
        P("dp", "sp", None),
        P(None, "sp"),
        P(),
        P(),
        P("sp"),
        P(),
        P("dp", None),
    )
    return jax.shard_map(
        step, mesh=mesh, in_specs=placed, out_specs=P("dp", "sp", None), check_vma=False
    )
```

```python
import jax
import jax.numpy as jnp
from jax import lax
from jax.experimental import pallas as pl
from jax.experimental.pallas import tpu as pltpu
from jax.sharding import PartitionSpec as P


HEAD_DIM = 64
STATE = 128
RATIO = 4
WIDTH = RATIO * HEAD_DIM
NORM_EPS = 1.0
HIGHEST = lax.Precision.HIGHEST
F32 = jnp.float32
BF16 = jnp.bfloat16
HALO = 4
EXTRA = 8
REACH = 3
COMMON = 16
PAD = 8
MIB = 1 << 20
OUT_LIMIT = 20 * MIB


def silu(u):
    half = 0.5 * u
    return half + half * jnp.tanh(half)


def lanes(first, size):
    return pl.ds(pl.multiple_of(first, STATE), size)


def conv_silu(pad_ref, halo, own, given, side, taps):
    tokens = own.shape[0]
    rows = 2 * tokens
    pad_ref[PAD - HALO : PAD, :] = halo.astype(F32)
    pad_ref[pl.ds(pl.multiple_of(PAD + side * tokens, 8), tokens), :] = own.astype(F32)
    pad_ref[pl.ds(pl.multiple_of(PAD + (1 - side) * tokens, 8), tokens), :] = given.astype(F32)
    total = taps[3:4, :] * pad_ref[PAD : PAD + rows, :]
    for back in range(1, 4):
        total = total + taps[3 - back : 4 - back, :] * pad_ref[PAD - back : PAD - back + rows, :]
    return silu(total)


def per_head(columns, first):
    tokens = columns.shape[0]
    lane = lax.broadcasted_iota(jnp.int32, (tokens, 128), 1)
    left = jnp.broadcast_to(columns[:, first : first + 1], (tokens, 128))
    right = jnp.broadcast_to(columns[:, first + 1 : first + 2], (tokens, 128))
    return jnp.where(lane < HEAD_DIM, left, right)


def head_row(values):
    lane = lax.broadcasted_iota(jnp.int32, (1, WIDTH), 1)
    row = jnp.broadcast_to(values[0:1], (1, WIDTH))
    for head in range(1, RATIO):
        row = jnp.where(
            lane >= head * HEAD_DIM, jnp.broadcast_to(values[head : head + 1], (1, WIDTH)), row
        )
    return row


def steps_of(raw):
    tokens = raw.shape[1]
    raw = raw.astype(F32)
    dt = jnp.maximum(raw, 0.0) + jnp.log1p(jnp.exp(-jnp.abs(raw)))
    src = lax.broadcasted_iota(jnp.int32, (tokens, tokens), 0)
    dst = lax.broadcasted_iota(jnp.int32, (tokens, tokens), 1)
    upper = (src <= dst).astype(F32)
    return dt, jnp.dot(dt, upper, precision=HIGHEST, preferred_element_type=F32)


def thirds(value):
    high = value.astype(BF16).astype(F32)
    rest = value - high
    middle = rest.astype(BF16).astype(F32)
    return [high, middle, rest - middle]


def share_kernel(
    logs_ref, raw_ref, taps_ref, x_ref, b_ref, c_ref,
    small_ref, dt_ref, own_ref, give_ref, own_c_ref, give_c_ref,
):
    heads, tokens = raw_ref.shape
    side = lax.rem(lax.axis_index("sp"), 2)
    other = 1 - side
    raw = raw_ref[...].astype(F32)
    left = 0
    for source in (x_ref, b_ref):
        half = source.shape[1] // 2
        own_ref[:, left : left + half] = source[:, lanes(side * half, half)]
        give_ref[0:tokens, left : left + half] = source[:, lanes(other * half, half)]
        left += half
    half = c_ref.shape[1] // 2
    own_c_ref[...] = c_ref[:, lanes(side * half, half)]
    give_c_ref[...] = c_ref[:, lanes(other * half, half)]
    theirs = jnp.where(other == 0, raw[0 : heads // 2], raw[heads // 2 :])
    per = left // tokens
    flats = []
    for first in range(0, heads // 2, per):
        held = min(per, heads // 2 - first)
        flats.append(
            jnp.concatenate(
                [theirs[first + k : first + k + 1] for k in range(held)]
                + [jnp.zeros((1, tokens), F32)] * (per - held),
                axis=1,
            )
        )
    flats.append(jnp.zeros((EXTRA - len(flats), left), F32))
    give_ref[tokens : tokens + EXTRA, :] = jnp.concatenate(flats, axis=0).astype(BF16)

    dt, prefix = steps_of(raw)
    for group in range(heads // RATIO):
        rows = slice(group * RATIO, (group + 1) * RATIO)
        dt_ref[group, 0:RATIO, :] = prefix[rows]
        dt_ref[group, RATIO:, :] = dt[rows]
    ones = jnp.ones((8, tokens), F32)
    sums = lax.dot_general(
        ones, dt, (((1,), (1,)), ((), ())), precision=HIGHEST, preferred_element_type=F32
    )
    sums = jnp.concatenate([sums[0:1], jnp.zeros((1, 128 - heads), F32)], axis=1)
    common = jnp.concatenate(
        [taps_ref[...].astype(F32)]
        + thirds(jnp.broadcast_to(logs_ref[:, 0:1], (1, 128)))
        + thirds(jnp.broadcast_to(logs_ref[:, 1:2], (1, 128)))
        + thirds(sums)
        + [jnp.zeros((3, 128), F32)],
        axis=0,
    ).astype(BF16)
    ends = []
    for part in range(2):
        rows = []
        tails = [ref[tokens - 8 :, :].astype(F32) for ref in (x_ref, b_ref, c_ref)]
        for token in range(8 - REACH, 8):
            for tail in tails:
                half = tail.shape[1] // 2
                for first in range(part * half, (part + 1) * half, STATE):
                    rows.append(tail[token : token + 1, first : first + STATE])
        ends.append(jnp.concatenate(rows, axis=0).astype(BF16))
    for rank in range(small_ref.shape[0]):
        small_ref[rank, 0:COMMON, :] = common
        small_ref[rank, COMMON:, :] = ends[rank % 2]


def halo_of(shared_ref, first, count):
    pair = lax.axis_index("sp") // 2
    source = jnp.maximum(2 * pair - 1, 0)
    ends = shared_ref[source, COMMON:, :].astype(F32)
    ends = jnp.where(pair == 0, 0.0, ends)
    stride = ends.shape[0] // REACH
    row_id = lax.broadcasted_iota(jnp.int32, ends.shape, 0)
    rows = [jnp.zeros((HALO - REACH, count * STATE), F32)]
    for token in range(REACH):
        picked = [
            jnp.sum(
                jnp.where(row_id == token * stride + first + k, ends, 0.0), axis=0, keepdims=True
            )
            for k in range(count)
        ]
        rows.append(jnp.concatenate(picked, axis=1))
    return jnp.concatenate(rows, axis=0)


def early_kernel(got_ref, dt_ref, steps_ref):
    side = lax.rem(lax.axis_index("sp"), 2)
    groups, _, tokens = steps_ref.shape
    flat = got_ref[...].astype(F32)
    per = flat.shape[1] // tokens
    raw = jnp.concatenate(
        [
            flat[k // per : k // per + 1, k % per * tokens : (k % per + 1) * tokens]
            for k in range(groups * RATIO)
        ],
        axis=0,
    )
    dt, prefix = steps_of(raw)
    for group in range(groups):
        rows = slice(group * RATIO, (group + 1) * RATIO)
        given = jnp.concatenate([prefix[rows], dt[rows]], axis=0)
        own = dt_ref[side * groups + group]
        steps_ref[group, 0 : 2 * RATIO, :] = jnp.where(side == 0, own, given)
        steps_ref[group, 2 * RATIO :, :] = jnp.where(side == 0, given, own)


def state_kernel(
    own_ref, own_b_ref, got_ref, got_b_ref, shared_ref, tb_ref, steps_ref,
    state_ref, first_ref, xin_ref, bin_ref, cum_ref, pad_ref, pad_b_ref,
):
    side = lax.rem(lax.axis_index("sp"), 2)
    tokens = own_ref.shape[0]
    end = tokens - 1
    per = steps_ref.shape[0]
    for k in range(per):
        wide = slice(k * WIDTH, (k + 1) * WIDTH)
        thin = slice(k * STATE, (k + 1) * STATE)
        group = per * pl.program_id(0) + k
        piece = 8 * side + 2 * group
        lower = shared_ref[piece, 0:COMMON, :].astype(F32)
        upper = shared_ref[piece + 1, 0:COMMON, :].astype(F32)
        rows = steps_ref[k]
        logs = []
        for part in (lower, upper):
            for row in (4, 7):
                logs.append(part[row : row + 1] + part[row + 1 : row + 2] + part[row + 2 : row + 3])
        rate = jnp.exp(jnp.concatenate(logs, axis=0))
        cums, tails = [], []
        for block in range(2):
            prefix = rows[8 * block : 8 * block + RATIO]
            dt = rows[8 * block + RATIO : 8 * block + 2 * RATIO]
            cum = -rate * prefix
            cums += [cum, dt]
            tails.append(jnp.exp(cum[:, end : end + 1] - cum) * dt)
        cum_ref[k] = jnp.concatenate(cums, axis=0)
        columns = jnp.transpose(jnp.concatenate(tails, axis=0))
        xin = conv_silu(
            pad_ref.at[k],
            halo_of(shared_ref, 2 * group, 2),
            own_ref[:, wide],
            got_ref[0:tokens, wide],
            side,
            jnp.concatenate([lower[0:4], upper[0:4]], axis=1),
        ).astype(BF16)
        bin_ = conv_silu(
            pad_b_ref.at[k],
            halo_of(shared_ref, 8 + group, 1),
            own_b_ref[:, thin],
            got_b_ref[0:tokens, thin],
            side,
            tb_ref[:, lanes((side * 4 + group) * STATE, STATE)].astype(F32),
        ).astype(BF16)
        bin_ref[:, thin] = bin_
        xin_ref[:, wide] = xin
        states = []
        for block in range(2):
            part = slice(block * tokens, (block + 1) * tokens)
            scale = jnp.concatenate(
                [per_head(columns, 4 * block), per_head(columns, 4 * block + 2)], axis=1
            )
            scaled = (xin[part].astype(F32) * scale).astype(BF16)
            states.append(
                lax.dot_general(
                    bin_[part],
                    scaled,
                    (((0,), (0,)), ((), ())),
                    preferred_element_type=F32,
                )
            )
        both = (states[1] + states[0] * head_row(jnp.exp(cums[2][:, end : end + 1]))).astype(BF16)
        for half in range(2):
            cols = slice(half * STATE, (half + 1) * STATE)
            first_ref[2 * k + half] = states[0][:, cols].astype(BF16)
            for part in range(2):
                state_ref[4 * k + 2 * half + part] = both[
                    part * HEAD_DIM : (part + 1) * HEAD_DIM, cols
                ]


def inner_kernel(
    own_ref, got_ref, shared_ref, tc_ref, bin_ref, xin_ref, cum_ref,
    cin_ref, inner_ref, pad_ref,
):
    side = lax.rem(lax.axis_index("sp"), 2)
    group = pl.program_id(0)
    groups = pl.num_programs(0)
    tokens = own_ref.shape[0]
    cin = conv_silu(
        pad_ref,
        halo_of(shared_ref, 12 + group, 1),
        own_ref[...],
        got_ref[...],
        side,
        tc_ref[:, lanes((side * groups + group) * STATE, STATE)].astype(F32),
    ).astype(BF16)
    cin_ref[...] = cin
    row_id = lax.broadcasted_iota(jnp.int32, (tokens, tokens), 0)
    col_id = lax.broadcasted_iota(jnp.int32, (tokens, tokens), 1)
    causal = row_id >= col_id
    for block in range(2):
        part = slice(block * tokens, (block + 1) * tokens)
        scores = lax.dot_general(
            cin[part], bin_ref[part, :], (((1,), (1,)), ((), ())), preferred_element_type=F32
        )
        rows = cum_ref[0, 8 * block : 8 * block + 8, :]
        columns = jnp.transpose(rows)
        for head in range(RATIO):
            spread = columns[:, head : head + 1] - rows[head : head + 1, :]
            decay = jnp.exp(jnp.where(causal, spread, -jnp.inf))
            weights = (scores * decay * rows[RATIO + head : RATIO + head + 1, :]).astype(BF16)
            cols = slice(head * HEAD_DIM, (head + 1) * HEAD_DIM)
            inner_ref[part, cols] = jnp.dot(
                weights, xin_ref[part, cols], preferred_element_type=F32
            )


def scan_kernel(shared_ref, local_ref, out_ref):
    me = lax.axis_index("sp")
    pair = me // 2
    count = local_ref.shape[0]
    sums = jnp.concatenate(
        [
            jnp.sum(shared_ref[rank, 0:COMMON, :].astype(F32)[10:13], axis=0, keepdims=True)
            for rank in range(count)
        ],
        axis=0,
    )
    lane = lax.broadcasted_iota(jnp.int32, sums.shape, 1)
    for upper in range(2):
        ends = []
        for head in range(2):
            mine = jnp.sum(
                jnp.where(lane == count * upper + 2 * pair + head, sums, 0.0),
                axis=1,
                keepdims=True,
            )
            logs = shared_ref[8 * upper + pair, 0:COMMON, :].astype(F32)
            logs = logs[4 + 3 * head : 7 + 3 * head]
            rate = jnp.exp(logs[0:1] + logs[1:2] + logs[2:3])
            ends.append(jnp.exp(-rate * mine))
        decay = jnp.where(lane < HEAD_DIM, ends[0], ends[1])
        entering = jnp.zeros(local_ref.shape[1:], F32)
        for step in range(count // 2):
            slot = 2 * step + upper
            out_ref[slot] = entering.astype(BF16)
            if step + 1 < count // 2:
                passed = decay[2 * step : 2 * step + 1, :] * decay[2 * step + 1 : 2 * step + 2, :]
                entering = entering * passed + local_ref[slot].astype(F32)


def core_of(block, pair, ent_ref, first_ref, cin_ref, inner_ref, cum_ref):
    tokens = cin_ref.shape[0]
    group, half = pair // 2, pair % 2
    rows = cum_ref[group]
    picked = jnp.where(block == 0, rows[0:8], rows[8:16])
    columns = jnp.transpose(jnp.exp(picked))
    cols = slice(half * STATE, (half + 1) * STATE)
    passed = head_row(jnp.exp(rows[0:RATIO, tokens - 1 : tokens]))[:, cols]
    entering = ent_ref[pair].astype(F32) * jnp.where(block == 0, 1.0, passed) + jnp.where(
        block == 0, 0.0, first_ref[pair].astype(F32)
    )
    carried = jnp.dot(
        cin_ref[:, group * STATE : (group + 1) * STATE],
        entering.astype(BF16),
        preferred_element_type=F32,
    )
    inner = inner_ref[:, pair * STATE : (pair + 1) * STATE]
    return (inner + carried * per_head(columns, 2 * half)).astype(BF16)


def average_of():
    row_id = lax.broadcasted_iota(jnp.int32, (STATE, STATE), 0) // HEAD_DIM
    col_id = lax.broadcasted_iota(jnp.int32, (STATE, STATE), 1) // HEAD_DIM
    return jnp.where(row_id == col_id, 1.0 / HEAD_DIM, 0.0).astype(BF16)


def gate_norm(core, gate, gain, average):
    v = core.astype(F32) * silu(gate.astype(F32))
    squares = v * v
    high = squares.astype(BF16)
    low = (squares - high.astype(F32)).astype(BF16)
    mean = jnp.dot(high, average, preferred_element_type=F32) + jnp.dot(
        low, average, preferred_element_type=F32
    )
    return v * lax.rsqrt(mean + NORM_EPS) * gain


def give_kernel(ent_ref, first_ref, cin_ref, inner_ref, cum_ref, core_ref):
    block = 1 - lax.rem(lax.axis_index("sp"), 2)
    for pair in range(ent_ref.shape[0]):
        core_ref[:, pair * STATE : (pair + 1) * STATE] = core_of(
            block, pair, ent_ref, first_ref, cin_ref, inner_ref, cum_ref
        )


def mine_kernel(
    ent_ref, first_ref, cin_ref, inner_ref, cum_ref, z_ref, gain_ref, normed_ref
):
    side = lax.rem(lax.axis_index("sp"), 2)
    average = average_of()
    pairs = ent_ref.shape[0]
    for pair in range(pairs):
        core = core_of(side, pair, ent_ref, first_ref, cin_ref, inner_ref, cum_ref)
        cols = lanes((side * pairs + pair) * STATE, STATE)
        normed_ref[pair] = gate_norm(core, z_ref[:, cols], gain_ref[:, cols], average).astype(BF16)


def join_kernel(a_ref, b_ref, c_ref, d_ref, out_ref):
    rows = a_ref.shape[0]
    for k, ref in enumerate((a_ref, b_ref, c_ref, d_ref)):
        out_ref[k * rows : (k + 1) * rows, :] = ref[...]


def hold_kernel(*refs):
    pieces, held_ref, sems = refs[:8], refs[8], refs[9]
    deep = pieces[0].shape[0]
    copies = [
        pltpu.make_async_copy(ref, held_ref.at[k * deep : (k + 1) * deep, :], sems.at[k])
        for k, ref in enumerate(pieces)
    ]
    for copy in copies:
        copy.start()
    for copy in copies:
        copy.wait()


def out_kernel(core_ref, near_ref, z_ref, gain_ref, held_ref, out_ref, normed_ref, ordered_ref):
    rank = lax.axis_index("dp")
    y, x, core = rank // 8, lax.rem(rank // 2, 4), lax.rem(rank, 2)
    side = lax.rem(lax.axis_index("sp"), 2)
    average = average_of()
    pairs = near_ref.shape[0]
    for pair in range(pairs):
        normed_ref[side * pairs + pair] = near_ref[pair].astype(F32)
        far = (1 - side) * pairs + pair
        cols = lanes(far * STATE, STATE)
        value = gate_norm(
            core_ref[:, pair * STATE : (pair + 1) * STATE],
            z_ref[:, cols],
            gain_ref[:, cols],
            average,
        )
        normed_ref[far] = value
    tokens = out_ref.shape[0]
    lane = lax.broadcasted_iota(jnp.int32, (tokens, STATE), 1)

    def chip(side, position):
        major, minor = position // 4, position % 4
        ry = jnp.where(side == 0, major, minor)
        rx = jnp.where(side == 0, minor, major)
        return lax.rem(y + 4 - ry, 4) * 4 + lax.rem(x + 4 - rx, 4)

    for half, side in enumerate((core, 1 - core)):
        for k in range(8):
            left = normed_ref[chip(side, 2 * k)]
            right = normed_ref[chip(side, 2 * k + 1)]
            turned = pltpu.roll(jnp.where(side == 0, right, left), HEAD_DIM, 1)
            left = jnp.where(side == 0, left, turned)
            right = jnp.where(side == 0, turned, right)
            first = (half * 8 + k) * STATE
            ordered_ref[:, first : first + STATE] = jnp.where(
                lane < HEAD_DIM, left, right
            ).astype(BF16)
    chunk = 512
    for first in range(0, out_ref.shape[1], chunk):
        cols = slice(first, first + chunk)
        out_ref[:, cols] = jnp.dot(
            ordered_ref[...], held_ref[:, cols], preferred_element_type=F32
        ).astype(BF16)


def vmem():
    return pl.BlockSpec(memory_space=pltpu.VMEM)


def in_hbm(*values):
    return [pltpu.with_memory_space_constraint(v, pltpu.HBM) for v in values]


def cost(flops, moved, special):
    return pl.CostEstimate(flops=flops, bytes_accessed=moved, transcendentals=special)


def first_step(y, x, core, d):
    return (y, x + d, core) if core == 0 else (y + d, x, core)


def second_step(y, x, core, d):
    return (y + d, x, core) if core == 0 else (y, x + d, core)


def swap_step(y, x, core, d):
    return y, x, 1 - core


def torus(step, d):
    pairs = []
    for rank in range(32):
        y, x, core = step(rank // 8, rank // 2 % 4, rank % 2, d)
        pairs.append((rank, ((y % 4) * 4 + x % 4) * 2 + core))
    return pairs


def step(
    stream_x, stream_b, stream_c, gate_z, step_raw,
    conv_x, conv_b, conv_c, decay_log, norm_gain, w_out,
):
    ranks = lax.axis_size("sp")
    x, b, c, z, raw = (v[0] for v in (stream_x, stream_b, stream_c, gate_z, step_raw))
    tokens, inner_width = x.shape
    wide, thin = inner_width // 2, b.shape[1] // 2
    groups = thin // STATE
    pairs = wide // STATE
    swap = [(i, i ^ 1) for i in range(ranks)]
    x, b, c, raw, taps, logs = in_hbm(
        x, b, c, jnp.transpose(raw), conv_x, decay_log[None]
    )

    cols = wide + thin
    small, dt, own, give, own_c, give_c = pl.pallas_call(
        share_kernel,
        in_specs=[vmem()] * 6,
        out_specs=[vmem()] * 6,
        out_shape=[
            jax.ShapeDtypeStruct((ranks, COMMON + REACH * (cols + thin) // STATE, STATE), BF16),
            jax.ShapeDtypeStruct((2 * groups, 2 * RATIO, tokens), F32),
            jax.ShapeDtypeStruct((tokens, cols), BF16),
            jax.ShapeDtypeStruct((tokens + EXTRA, cols), BF16),
            jax.ShapeDtypeStruct((tokens, thin), BF16),
            jax.ShapeDtypeStruct((tokens, thin), BF16),
        ],
        compiler_params=pltpu.CompilerParams(vmem_limit_bytes=8 * MIB),
        cost_estimate=cost(10_000_000, 2_000_000, 10_000),
        name="share",
    )(logs, raw, taps, x, b, c)
    shared = lax.all_to_all(small, "sp", 0, 0, tiled=True)
    got = lax.ppermute(give, "sp", swap)
    got_c = lax.ppermute(give_c, "sp", swap)

    w1, w2, w3 = (lax.ppermute(w_out, "dp", torus(first_step, d)) for d in (1, 2, 3))
    row = pl.pallas_call(
        join_kernel,
        in_specs=[vmem()] * 4,
        out_specs=vmem(),
        out_shape=jax.ShapeDtypeStruct((4 * w_out.shape[0], w_out.shape[1]), BF16),
        compiler_params=pltpu.CompilerParams(vmem_limit_bytes=8 * MIB),
        cost_estimate=cost(1_000_000, 2_000_000, 0),
        name="join",
    )(w_out, w1, w2, w3)
    mine = [row] + [lax.ppermute(row, "dp", torus(second_step, d)) for d in (1, 2, 3)]
    other = [lax.ppermute(v, "dp", torus(swap_step, 0)) for v in mine]

    steps = pl.pallas_call(
        early_kernel,
        grid=(1,),
        in_specs=[
            pl.BlockSpec((EXTRA, cols), lambda i: (tokens // EXTRA, 0)),
            pl.BlockSpec(dt.shape, lambda i: (0, 0, 0)),
        ],
        out_specs=pl.BlockSpec((groups, 4 * RATIO, tokens), lambda i: (0, 0, 0)),
        out_shape=jax.ShapeDtypeStruct((groups, 4 * RATIO, tokens), F32),
        compiler_params=pltpu.CompilerParams(vmem_limit_bytes=8 * MIB),
        cost_estimate=cost(100_000_000, 100_000, 20_000),
        name="early",
    )(got, dt)

    per = 2
    away = wide // (per * STATE)
    state, first, xin, bin_, cum = pl.pallas_call(
        state_kernel,
        grid=(groups // per,),
        in_specs=[
            pl.BlockSpec((tokens, per * WIDTH), lambda g: (0, g)),
            pl.BlockSpec((tokens, per * STATE), lambda g: (0, away + g)),
            pl.BlockSpec((tokens + EXTRA, per * WIDTH), lambda g: (0, g)),
            pl.BlockSpec((tokens + EXTRA, per * STATE), lambda g: (0, away + g)),
            pl.BlockSpec(shared.shape, lambda g: (0, 0, 0)),
            pl.BlockSpec((4, 2 * thin), lambda g: (0, 0)),
            pl.BlockSpec((per, 4 * RATIO, tokens), lambda g: (g, 0, 0)),
        ],
        out_specs=[
            pl.BlockSpec((4 * per, HEAD_DIM, STATE), lambda g: (g, 0, 0)),
            pl.BlockSpec((2 * per, STATE, STATE), lambda g: (g, 0, 0)),
            pl.BlockSpec((2 * tokens, per * WIDTH), lambda g: (0, g)),
            pl.BlockSpec((2 * tokens, per * STATE), lambda g: (0, g)),
            pl.BlockSpec((per, 4 * RATIO, tokens), lambda g: (g, 0, 0)),
        ],
        out_shape=[
            jax.ShapeDtypeStruct((ranks, HEAD_DIM, STATE), BF16),
            pltpu.HBM((pairs, STATE, STATE), BF16),
            pltpu.HBM((2 * tokens, wide), BF16),
            pltpu.HBM((2 * tokens, thin), BF16),
            pltpu.HBM((groups, 4 * RATIO, tokens), F32),
        ],
        scratch_shapes=[
            pltpu.VMEM((per, PAD + 2 * tokens, WIDTH), F32),
            pltpu.VMEM((per, PAD + 2 * tokens, STATE), F32),
        ],
        compiler_params=pltpu.CompilerParams(vmem_limit_bytes=16 * MIB),
        cost_estimate=cost(4_000_000_000, 2_000_000, 400_000),
        name="state",
    )(own, own, got, got, shared, conv_b, steps)

    local = lax.all_to_all(state, "sp", 0, 0, tiled=True)

    cin, inner = pl.pallas_call(
        inner_kernel,
        grid=(groups,),
        in_specs=[
            pl.BlockSpec((tokens, STATE), lambda g: (0, g)),
            pl.BlockSpec((tokens, STATE), lambda g: (0, g)),
            pl.BlockSpec(shared.shape, lambda g: (0, 0, 0)),
            pl.BlockSpec((4, 2 * thin), lambda g: (0, 0)),
            pl.BlockSpec((2 * tokens, STATE), lambda g: (0, g)),
            pl.BlockSpec((2 * tokens, WIDTH), lambda g: (0, g)),
            pl.BlockSpec((1, 4 * RATIO, tokens), lambda g: (g, 0, 0)),
        ],
        out_specs=[
            pl.BlockSpec((2 * tokens, STATE), lambda g: (0, g)),
            pl.BlockSpec((2 * tokens, WIDTH), lambda g: (0, g)),
        ],
        out_shape=[
            pltpu.HBM((2 * tokens, thin), BF16),
            pltpu.HBM((2 * tokens, wide), F32),
        ],
        scratch_shapes=[pltpu.VMEM((PAD + 2 * tokens, STATE), F32)],
        compiler_params=pltpu.CompilerParams(vmem_limit_bytes=16 * MIB),
        cost_estimate=cost(4_000_000_000, 2_000_000, 700_000),
        name="inner",
    )(own_c, got_c, shared, conv_c, *in_hbm(bin_, xin, cum))

    entering = pl.pallas_call(
        scan_kernel,
        in_specs=[vmem(), vmem()],
        out_specs=vmem(),
        out_shape=jax.ShapeDtypeStruct(local.shape, BF16),
        compiler_params=pltpu.CompilerParams(vmem_limit_bytes=8 * MIB),
        cost_estimate=cost(1_000_000_000, 1_000_000, 0),
        name="scan",
    )(shared, local)
    entering = lax.all_to_all(entering, "sp", 0, 0, tiled=True)
    entering = entering.reshape(pairs, STATE, STATE)

    mixer = (entering, *in_hbm(first, cin, inner, cum))

    def whole(value):
        return pl.BlockSpec(value.shape, lambda i: (0,) * value.ndim)

    def half_of(value, theirs):
        def index(i):
            side = lax.rem(lax.axis_index("sp"), 2)
            return (1 - side if theirs else side, 0)

        return pl.BlockSpec((value.shape[0] // 2, value.shape[1]), index)

    def mixer_specs(theirs):
        return [
            whole(entering),
            whole(first),
            half_of(cin, theirs),
            half_of(inner, theirs),
            whole(cum),
        ]

    core = pl.pallas_call(
        give_kernel,
        grid=(1,),
        in_specs=mixer_specs(True),
        out_specs=pl.BlockSpec((tokens, wide), lambda i: (0, 0)),
        out_shape=jax.ShapeDtypeStruct((tokens, wide), BF16),
        compiler_params=pltpu.CompilerParams(vmem_limit_bytes=8 * MIB),
        cost_estimate=cost(1_000_000_000, 1_000_000, 0),
        name="give",
    )(*mixer)
    got_core = lax.ppermute(core, "sp", swap)
    gain = norm_gain[None]
    normed = pl.pallas_call(
        mine_kernel,
        grid=(1,),
        in_specs=mixer_specs(False) + [whole(z), whole(gain)],
        out_specs=pl.BlockSpec((pairs, tokens, STATE), lambda i: (0, 0, 0)),
        out_shape=jax.ShapeDtypeStruct((pairs, tokens, STATE), BF16),
        compiler_params=pltpu.CompilerParams(vmem_limit_bytes=8 * MIB),
        cost_estimate=cost(2_000_000_000, 1_000_000, 0),
        name="mine",
    )(*mixer, *in_hbm(z, gain))
    held = pl.pallas_call(
        hold_kernel,
        in_specs=[pl.BlockSpec(memory_space=pl.ANY)] * 8,
        out_specs=pl.BlockSpec(memory_space=pltpu.VMEM),
        out_shape=pltpu.VMEM((inner_width, w_out.shape[1]), BF16),
        scratch_shapes=[pltpu.SemaphoreType.DMA((8,))],
        compiler_params=pltpu.CompilerParams(vmem_limit_bytes=16 * MIB),
        cost_estimate=cost(1_000_000, 16_000_000, 0),
        name="hold",
    )(*in_hbm(*mine), *other)
    mixed = pl.pallas_call(
        out_kernel,
        in_specs=[vmem()] * 5,
        out_specs=vmem(),
        out_shape=jax.ShapeDtypeStruct((tokens, w_out.shape[1]), BF16),
        scratch_shapes=[
            pltpu.VMEM((2 * pairs, tokens, STATE), F32),
            pltpu.VMEM((tokens, inner_width), BF16),
        ],
        compiler_params=pltpu.CompilerParams(vmem_limit_bytes=OUT_LIMIT),
        cost_estimate=cost(4_000_000_000, 10_000_000, 300_000),
        name="project",
    )(got_core, normed, z, gain, held)
    return mixed[None]


def solution(mesh):
    placed = (
        P("dp", "sp", None),
        P("dp", "sp", None),
        P("dp", "sp", None),
        P("dp", "sp", None),
        P("dp", "sp", None),
        P(None, "sp"),
        P(),
        P(),
        P("sp"),
        P(),
        P("dp", None),
    )
    return jax.shard_map(
        step, mesh=mesh, in_specs=placed, out_specs=P("dp", "sp", None), check_vma=False
    )
```
